256 devices in a mesh: grp: 2 (over z), fs: 16 (over y, core), tp: 8 (over x).
Axes of the slice: x: 8, y: 8, z: 2, core: 2. Of those that a mesh axis runs over, the one named last changes fastest.
The devices are a block of a 8x8x16 slice.
Arguments:
- stream: bfloat16 [32768, 2048], P(('grp', 'fs', 'tp')), parts along dimension 0, may hold values from -4 to 4
- gain_first: bfloat16 [2048], replicated, may hold values from 0.099609375 to 1.8984375
- gate_first: bfloat16 [2048, 4096], P('fs', 'tp'), may hold values from -0.125 to 0.125
- up_first: bfloat16 [2048, 4096], P('fs', 'tp'), may hold values from -0.125 to 0.125
- down_first: bfloat16 [4096, 2048], P('tp', 'fs'), may hold values from -0.09375 to 0.09375
- gain_second: bfloat16 [2048], replicated, may hold values from 0.099609375 to 1.8984375
- gate_second: bfloat16 [2048, 4096], P('fs', 'tp'), may hold values from -0.125 to 0.125
- up_second: bfloat16 [2048, 4096], P('fs', 'tp'), may hold values from -0.125 to 0.125
- down_second: bfloat16 [4096, 2048], P('tp', 'fs'), may hold values from -0.09375 to 0.09375
Outputs:
- result: bfloat16 [32768, 2048], P(('grp', 'fs', 'tp')), parts along dimension 0
The draws below stay inside these ranges and needn't reach their ends.
There are 2 independent parts, one for each index of `grp`. The reference program is written for one: setup_inputs(seed, part) draws one part's arguments, and reference() takes and returns one part's arrays. A program takes and returns all parts, laid end to end along the dimension named above; an argument that names none is the same for every part. Nothing has to cross between parts.
All inputs are finite; a program needn't handle non-finite values.
Results may differ from the reference program's by a relative error of at most 0.018.
Values may be sent and summed in bfloat16 or wider, within the bound.
A program may use at most 64 MiB of HBM per device.

```python
import jax
import jax.numpy as jnp
from jax import lax

D = 2048
FF = 4096
TOKENS = 16384
N_TP = 8


def block_scale(rng, extent, shards, smallest, largest):
    level = 1.0
    for position, blocks in shards:
        steps = jax.random.uniform(jax.random.fold_in(jax.random.fold_in(rng, 6), position), (blocks,), jnp.float32, smallest / len(shards), largest / len(shards))
        level = level * jnp.repeat(jnp.exp(steps), extent[position] // blocks).reshape((-1,) + (1,) * (len(extent) - 1 - position))
    return level


def scatter_about(stream_key, dims, deviation, bound, cuts=(), kind=jnp.bfloat16):
    drawn = deviation * jax.random.normal(stream_key, dims, jnp.float32)
    if cuts:
        drawn = drawn * block_scale(stream_key, dims, cuts, -0.22, 0.18)
    return jnp.clip(drawn, -bound, bound).astype(kind)


def setup_inputs(seed: int = 0, part: int = 0) -> dict:
    streams_of = jax.random.split(jax.random.key(seed), 10)
    part_keys = jax.random.split(jax.random.fold_in(streams_of[9], part), 10)
    return {
        "stream": scatter_about(part_keys[0], (TOKENS, D), 0.5, 4.0, ((0, 128),)),
        "gain_first": jnp.clip(1.0 + 0.18 * jax.random.normal(streams_of[1], (D,), jnp.float32), 0.099609375, 1.8984375).astype(jnp.bfloat16),
        "gate_first": scatter_about(streams_of[2], (D, FF), D ** -0.5, 0.125, ((0, 16), (1, 8))),
        "up_first": scatter_about(streams_of[3], (D, FF), D ** -0.5, 0.125, ((0, 16), (1, 8))),
        "down_first": scatter_about(streams_of[4], (FF, D), FF ** -0.5, 0.09375, ((0, 8), (1, 16))),
        "gain_second": jnp.clip(1.0 + 0.18 * jax.random.normal(streams_of[5], (D,), jnp.float32), 0.099609375, 1.8984375).astype(jnp.bfloat16),
        "gate_second": scatter_about(streams_of[6], (D, FF), D ** -0.5, 0.125, ((0, 16), (1, 8))),
        "up_second": scatter_about(streams_of[7], (D, FF), D ** -0.5, 0.125, ((0, 16), (1, 8))),
        "down_second": scatter_about(streams_of[8], (FF, D), FF ** -0.5, 0.09375, ((0, 8), (1, 16))),
    }


def half_branch(stream, gain, w_gate, w_up, w_down):
    stream_f = stream.astype(jnp.float32)
    normed = (stream_f * lax.rsqrt(lax.optimization_barrier(jnp.mean(stream_f * stream_f, axis=-1, keepdims=True)) + 1e-06) * gain.astype(jnp.float32)).astype(jnp.bfloat16)
    gate_act = jnp.dot(normed, w_gate, preferred_element_type=jnp.float32)
    up_act = jnp.dot(normed, w_up, preferred_element_type=jnp.float32)
    hidden = (jax.nn.silu(gate_act) * up_act).astype(jnp.bfloat16)
    span_width = FF // N_TP
    summed = jnp.zeros(stream.shape, jnp.float32)
    for shard in range(N_TP):
        partial_sum = jnp.dot(hidden[:, shard * span_width:(shard + 1) * span_width], w_down[shard * span_width:(shard + 1) * span_width], preferred_element_type=jnp.float32).astype(jnp.bfloat16)
        partial_sum = lax.optimization_barrier(partial_sum)
        summed = summed + partial_sum.astype(jnp.float32)
    return (stream_f + 0.5 * summed).astype(jnp.bfloat16)

def reference(stream, gain_first, gate_first, up_first, down_first, gain_second, gate_second, up_second, down_second):
    middle = half_branch(stream, gain_first, gate_first, up_first, down_first)
    return half_branch(middle, gain_second, gate_second, up_second, down_second)
```

```python
import functools

import jax
import jax.numpy as jnp
from jax import lax
from jax.experimental import pallas as pl
from jax.experimental.pallas import tpu as pltpu
from jax.sharding import PartitionSpec as P

MESH = pl.DeviceIdType.MESH
F32 = jnp.float32
BF16 = jnp.bfloat16
SUBS = 4
CORES = 2


def rms_norm(rows_f, gain):
    scale = lax.rsqrt(jnp.mean(rows_f * rows_f, axis=-1, keepdims=True) + 1e-06)
    return (rows_f * scale * gain.astype(F32)).astype(BF16)


def kernel(
    n_x, n_y,
    stream, gain1, g1, u1, d1, gain2, g2, u2, d2,
    out,
    wg, wu, wd, st, x1, p1, s1, mid, x2, p2, s2, rg, ru, rd, hid, res,
    load_sem, ag1_recv, rs1_recv, ag2_recv, rs2_recv, y_recv, sib_recv, rel_recv, fin_recv,
    ag1_send, rs1_send, ag2_send, rs2_send, y_send, sib_send, rel_send, fin_send, out_sem,
):
    x = lax.axis_index("tp")
    f = lax.axis_index("fs")
    y = f // CORES
    c = f % CORES
    d = 1 - 2 * c
    hops = n_x - 1
    wide = n_x // 2
    leap = n_x // 4
    rows = st.shape[0]
    sub = rows // SUBS
    shard = g1.shape[0]
    y_hops = n_y - 1
    per_set = 3 * y_hops

    x_next = {"tp": (x + d + n_x) % n_x}
    x_prev = {"tp": (x - d + n_x) % n_x}
    x_leap = {"tp": (x + leap * d + n_x) % n_x}
    x_leap_back = {"tp": (x - leap * d + n_x) % n_x}
    y_next = {"fs": CORES * ((y + d + n_y) % n_y) + c}
    y_prev = {"fs": CORES * ((y - d + n_y) % n_y) + c}
    sibling = {"fs": CORES * y + 1 - c}

    def remote(src, dst, send, recv, device):
        return pltpu.make_async_remote_copy(
            src_ref=src, dst_ref=dst, send_sem=send, recv_sem=recv,
            device_id=device, device_id_type=MESH,
        )

    def piece(w, mat, owner):
        span = pl.ds(pl.multiple_of(owner * shard, shard), shard)
        if mat == 0:
            return wg.at[w, span, :]
        if mat == 1:
            return wu.at[w, span, :]
        return wd.at[w, :, span]

    def many(w, mat, count):
        span = pl.ds(0, count * shard)
        if mat == 0:
            return wg.at[w, span, :]
        if mat == 1:
            return wu.at[w, span, :]
        return wd.at[w, :, span]

    def tok(ref, k, m):
        return ref.at[k, pl.ds(m * sub, sub), :]

    loads = [pltpu.make_async_copy(stream, st, load_sem.at[0])]
    for i, (src, w, mat) in enumerate(
        ((g1, 0, 0), (u1, 0, 1), (d1, 0, 2), (g2, 1, 0), (u2, 1, 1), (d2, 1, 2))
    ):
        loads.append(pltpu.make_async_copy(src, piece(w, mat, f), load_sem.at[1 + i]))
    for copy in loads:
        copy.start()
    barrier = pltpu.get_barrier_semaphore()
    partners = [x_next, x_prev, y_next, y_prev, sibling]
    if leap > 1:
        partners += [x_leap, x_leap_back]
    for device in partners:
        pl.semaphore_signal(barrier, inc=1, device_id=device, device_id_type=MESH)
    pl.semaphore_wait(barrier, len(partners))

    def share(w, mat, owner):
        ref = piece(w, mat, owner)
        remote(ref, ref, sib_send.at[w * 3 + mat], sib_recv.at[w * 3 + mat], sibling).start()

    def pass_on(w, mat, owner, n):
        ref = piece(w, mat, owner)
        remote(ref, ref, y_send.at[w * 3 + mat], y_recv.at[n], y_next).start()

    def own(w, mat):
        if w == 2:
            ref = piece(2, mat, f)
            remote(ref, ref, fin_send.at[mat], fin_recv.at[mat], x_leap).wait_recv()
        pass_on(w, mat, f, w * per_set + mat)
        share(w, mat, f)

    def y_tick(n):
        w = n // per_set
        r = n % per_set
        step = r // 3
        owner = CORES * ((y - d * (step + 1) + CORES * n_y) % n_y) + c

        def arrived(mat):
            ref = piece(w, mat, owner)
            remote(ref, ref, y_send.at[w * 3 + mat], y_recv.at[n], y_next).wait_recv()

            @pl.when(step < y_hops - 1)
            def _():
                pass_on(w, mat, owner, n + 3)

            for done in range(2):
                @pl.when((step == y_hops - 1) & (w == done))
                def _():
                    own(done + 1, mat)

            share(w, mat, owner)

        for mat in range(3):
            @pl.when((n < 3 * per_set) & (r % 3 == mat))
            def _():
                arrived(mat)

    def wait_siblings(w):
        for mat in range(3):
            ref = many(w, mat, n_y)
            remote(ref, ref, sib_send.at[w * 3 + mat], sib_recv.at[w * 3 + mat], sibling).wait_recv()

    for mat in range(3):
        loads[1 + mat].wait()
        own(0, mat)

    loads[0].wait()
    for m in range(SUBS):
        part = pl.ds(m * sub, sub)
        x1[0, part, :] = rms_norm(st[part, :].astype(F32), gain1[...])
        remote(tok(x1, 0, m), tok(x1, 1, m), ag1_send, ag1_recv.at[m], x_next).start()

    relay = (rg, ru, rd)
    for mat in range(3):
        loads[4 + mat].wait()
        remote(piece(1, mat, f), relay[mat], rel_send.at[mat], rel_recv.at[mat], x_leap).start()

    def ag1_tick(k, m, last):
        remote(tok(x1, k, m), tok(x1, k, m), ag1_send, ag1_recv.at[(k - 1) * SUBS + m], x_next).wait_recv()
        if not last:
            remote(tok(x1, k, m), tok(x1, k + 1, m), ag1_send, ag1_recv.at[k * SUBS + m], x_next).start()

    relay_at = max(1, n_y // 2 - 1)

    def gather_first(k, carry):
        @pl.when(k == relay_at)
        def _():
            for mat in range(3):
                remote(relay[mat], relay[mat], rel_send.at[mat], rel_recv.at[mat], x_leap).wait_recv()
                remote(relay[mat], piece(2, mat, f), fin_send.at[mat], fin_recv.at[mat], x_leap).start()

        for m in range(SUBS):
            ag1_tick(k, m, False)
            y_tick((k - 1) * SUBS + m)
        return carry

    lax.fori_loop(1, hops, gather_first, 0)
    wait_siblings(0)

    def hidden_part(tokens, w, lo, width):
        gate = jnp.dot(tokens, wg[w, :, lo:lo + width], preferred_element_type=F32)
        up = jnp.dot(tokens, wu[w, :, lo:lo + width], preferred_element_type=F32)
        return ((gate / (1.0 + jnp.exp(-gate))) * up).astype(BF16)

    ff = wg.shape[2]
    feats = wd.shape[2]

    def first_quarter(k, m):
        if m < 2:
            width = ff // 2
            lo = m * width
            hid[0, :, lo:lo + width] = hidden_part(x1[k], 0, lo, width)
        else:
            width = feats // 2
            lo = (m - 2) * width
            p1[k, :, lo:lo + width] = jnp.dot(
                hid[0], wd[0, :, lo:lo + width], preferred_element_type=F32
            ).astype(BF16)

    def rs1_copy(src, k, m):
        return remote(src, tok(s1, k - 1, m), rs1_send, rs1_recv.at[(k - 1) * SUBS + m], x_next)

    def reduce_first(j, carry):
        for m in range(SUBS):
            @pl.when(j == 0)
            def _():
                ag1_tick(hops, m, True)

            @pl.when(j == 1)
            def _():
                rs1_copy(tok(p1, 1, m), 1, m).start()

            @pl.when(j >= 2)
            def _():
                part = pl.ds(m * sub, sub)
                rs1_copy(tok(s1, j - 2, m), j - 1, m).wait_recv()
                s1[j - 2, part, :] = (
                    s1[j - 2, part, :].astype(F32) + p1[j, part, :].astype(F32)
                ).astype(BF16)
                rs1_copy(tok(s1, j - 2, m), j, m).start()

            y_tick((hops - 1 + j) * SUBS + m)
            first_quarter((j + 1) % n_x, m)
        return carry

    lax.fori_loop(0, n_x, reduce_first, 0)

    for m in range(SUBS):
        part = pl.ds(m * sub, sub)
        rs1_copy(tok(s1, hops - 1, m), hops, m).wait_recv()
        total = s1[hops - 1, part, :].astype(F32) + p1[0, part, :].astype(F32)
        middle = (st[part, :].astype(F32) + 0.5 * total).astype(BF16)
        mid[part, :] = middle
        x2[0, part, :] = rms_norm(middle.astype(F32), gain2[...])
        remote(tok(x2, 0, m), tok(x2, 1, m), ag2_send, ag2_recv.at[m], x_next).start()
        y_tick((hops - 1 + n_x) * SUBS + m)

    def rest(n, carry):
        y_tick(n)
        return carry

    lax.fori_loop((hops + n_x) * SUBS, 3 * per_set, rest, 0)
    wait_siblings(1)
    wait_siblings(2)

    def second_quarter(k, m):
        if m < 2:
            width = ff // 2
            for lo in (0, width):
                hid[m, :, lo:lo + width] = hidden_part(x2[k], 1 + m, lo, width)
        else:
            width = feats // 2
            lo = (m - 2) * width
            p2[k, :, lo:lo + width] = (
                jnp.dot(hid[0], wd[1, :, lo:lo + width], preferred_element_type=F32)
                + jnp.dot(hid[1], wd[2, :, lo:lo + width], preferred_element_type=F32)
            ).astype(BF16)

    def gather_second(k, carry):
        for m in range(SUBS):
            @pl.when(k < wide)
            def _():
                remote(tok(x2, k, m), tok(x2, k, m), ag2_send, ag2_recv.at[(k - 1) * SUBS + m], x_next).wait_recv()

            @pl.when(k < wide - 1)
            def _():
                remote(tok(x2, k, m), tok(x2, k + 1, m), ag2_send, ag2_recv.at[k * SUBS + m], x_next).start()

            second_quarter(k - 1, m)
        return carry

    lax.fori_loop(1, wide + 1, gather_second, 0)

    def rs2_copy(src, k, m):
        return remote(src, tok(s2, k - 1, m), rs2_send, rs2_recv.at[(k - 1) * SUBS + m], x_prev)

    for m in range(SUBS):
        rs2_copy(tok(p2, wide - 1, m), wide - 1, m).start()

    for k in range(wide - 2, 0, -1):
        for m in range(SUBS):
            part = pl.ds(m * sub, sub)
            rs2_copy(tok(s2, k, m), k + 1, m).wait_recv()
            s2[k, part, :] = (
                s2[k, part, :].astype(F32) + p2[k, part, :].astype(F32)
            ).astype(BF16)
            rs2_copy(tok(s2, k, m), k, m).start()

    stores = []
    for m in range(SUBS):
        part = pl.ds(m * sub, sub)
        rs2_copy(tok(s2, 0, m), 1, m).wait_recv()
        total = s2[0, part, :].astype(F32) + p2[0, part, :].astype(F32)
        res[part, :] = (mid[part, :].astype(F32) + 0.5 * total).astype(BF16)
        copy = pltpu.make_async_copy(res.at[part, :], out.at[part, :], out_sem.at[m])
        copy.start()
        stores.append(copy)

    def sent(ref, sem):
        remote(ref, ref, sem, rel_recv.at[0], sibling).wait_send()

    sent(x1.at[pl.ds(0, hops)], ag1_send)
    sent(s1, rs1_send)
    sent(x2.at[pl.ds(0, wide - 1)], ag2_send)
    sent(s2, rs2_send)
    for mat in range(3):
        sent(relay[mat], rel_send.at[mat])
        sent(relay[mat], fin_send.at[mat])
        for w in range(3):
            sent(many(w, mat, y_hops), y_send.at[w * 3 + mat])
            sent(many(w, mat, n_y), sib_send.at[w * 3 + mat])
    for copy in stores:
        copy.wait()


def solution(mesh):
    n_x = mesh.shape["tp"]
    n_y = mesh.shape["fs"] // CORES

    def local(stream, gain1, g1, u1, d1, gain2, g2, u2, d2):
        rows, feats = stream.shape
        shard, ff = g1.shape
        wide = n_x // 2
        any_spec = pl.BlockSpec(memory_space=pl.ANY)
        vmem_spec = pl.BlockSpec(memory_space=pltpu.VMEM)
        dma = pltpu.SemaphoreType.DMA
        y_count = 9 * (n_y - 1)
        return pl.pallas_call(
            functools.partial(kernel, n_x, n_y),
            out_shape=jax.ShapeDtypeStruct((rows, feats), BF16),
            in_specs=[any_spec, vmem_spec, any_spec, any_spec, any_spec,
                      vmem_spec, any_spec, any_spec, any_spec],
            out_specs=any_spec,
            scratch_shapes=[
                pltpu.VMEM((3, feats, ff), BF16),
                pltpu.VMEM((3, feats, ff), BF16),
                pltpu.VMEM((3, ff, feats), BF16),
                pltpu.VMEM((rows, feats), BF16),
                pltpu.VMEM((n_x, rows, feats), BF16),
                pltpu.VMEM((n_x, rows, feats), BF16),
                pltpu.VMEM((n_x - 1, rows, feats), BF16),
                pltpu.VMEM((rows, feats), BF16),
                pltpu.VMEM((wide, rows, feats), BF16),
                pltpu.VMEM((wide, rows, feats), BF16),
                pltpu.VMEM((wide - 1, rows, feats), BF16),
                pltpu.VMEM((shard, ff), BF16),
                pltpu.VMEM((shard, ff), BF16),
                pltpu.VMEM((ff, shard), BF16),
                pltpu.VMEM((2, rows, ff), BF16),
                pltpu.VMEM((rows, feats), BF16),
                dma((7,)),
                dma(((n_x - 1) * SUBS,)),
                dma(((n_x - 1) * SUBS,)),
                dma(((wide - 1) * SUBS,)),
                dma(((wide - 1) * SUBS,)),
                dma((y_count,)),
                dma((9,)),
                dma((3,)),
                dma((3,)),
                dma,
                dma,
                dma,
                dma,
                dma((9,)),
                dma((9,)),
                dma((3,)),
                dma((3,)),
                dma((SUBS,)),
            ],
            compiler_params=pltpu.CompilerParams(
                collective_id=0, has_side_effects=True, vmem_limit_bytes=60 * 1024 * 1024
            ),
        )(stream, gain1.reshape(1, -1), g1, u1, d1, gain2.reshape(1, -1), g2, u2, d2)

    tokens = P(("grp", "fs", "tp"), None)
    rows_split, cols_split = P("fs", "tp"), P("tp", "fs")
    in_specs = (
        tokens,
        P(), rows_split, rows_split, cols_split,
        P(), rows_split, rows_split, cols_split,
    )
    return jax.shard_map(local, mesh=mesh, in_specs=in_specs, out_specs=tokens, check_vma=False)
```

```python
import functools

import jax
import jax.numpy as jnp
from jax import lax
from jax.experimental import pallas as pl
from jax.experimental.pallas import tpu as pltpu
from jax.sharding import PartitionSpec as P

MESH = pl.DeviceIdType.MESH
F32 = jnp.float32
BF16 = jnp.bfloat16
SUBS = 4
CORES = 2
LANES = 128


def rms_norm(rows_f, gain):
    scale = lax.rsqrt(jnp.mean(rows_f * rows_f, axis=-1, keepdims=True) + 1e-06)
    return (rows_f * scale * gain).astype(BF16)


def kernel(
    n_x, n_y,
    stream, gain1, g1, u1, d1, gain2, g2, u2, d2,
    out,
    wg, wu, wd, st, x1, p1, s1, mid, x2, p2, s2, rg, ru, rd, hid, gains,
    load_sem, ag1_recv, rs1_recv, ag2_recv, rs2_recv, y_recv, sib_recv, rel_recv, fin_recv,
    ag1_send, rs1_send, ag2_send, rs2_send, y_send, sib_send, rel_send, fin_send,
):
    x = lax.axis_index("tp")
    f = lax.axis_index("fs")
    y = f // CORES
    c = f % CORES
    d = 1 - 2 * c
    hops = n_x - 1
    wide = n_x // 2
    leap = n_x // 4
    rows = st.shape[0]
    sub = rows // SUBS
    shard = g1.shape[0]
    y_hops = n_y - 1
    per_set = 3 * y_hops

    x_next = {"tp": (x + d + n_x) % n_x}
    x_prev = {"tp": (x - d + n_x) % n_x}
    x_leap = {"tp": (x + leap * d + n_x) % n_x}
    x_leap_back = {"tp": (x - leap * d + n_x) % n_x}
    y_next = {"fs": CORES * ((y + d + n_y) % n_y) + c}
    y_prev = {"fs": CORES * ((y - d + n_y) % n_y) + c}
    sibling = {"fs": CORES * y + 1 - c}

    def remote(src, dst, send, recv, device):
        return pltpu.make_async_remote_copy(
            src_ref=src, dst_ref=dst, send_sem=send, recv_sem=recv,
            device_id=device, device_id_type=MESH,
        )

    def piece(w, mat, owner):
        span = pl.ds(pl.multiple_of(owner * shard, shard), shard)
        if mat == 0:
            return wg.at[w, span, :]
        if mat == 1:
            return wu.at[w, span, :]
        return wd.at[w, :, span]

    def many(w, mat, count):
        span = pl.ds(0, count * shard)
        if mat == 0:
            return wg.at[w, span, :]
        if mat == 1:
            return wu.at[w, span, :]
        return wd.at[w, :, span]

    def tok(ref, k, m):
        return ref.at[k, pl.ds(pl.multiple_of(m * sub, sub), sub), :]

    loads = [pltpu.make_async_copy(stream, st, load_sem.at[0])]
    for i, (src, w, mat) in enumerate(
        ((g1, 0, 0), (u1, 0, 1), (d1, 0, 2), (g2, 1, 0), (u2, 1, 1), (d2, 1, 2))
    ):
        loads.append(pltpu.make_async_copy(src, piece(w, mat, f), load_sem.at[1 + i]))
    for copy in loads:
        copy.start()
    for i, gain in enumerate((gain1, gain2)):
        for j in range(gain.shape[0]):
            gains[i, :, j * LANES:(j + 1) * LANES] = gain[j:j + 1, :].astype(F32)
    barrier = pltpu.get_barrier_semaphore()
    partners = [x_next, x_prev, y_next, y_prev, sibling]
    if leap > 1:
        partners += [x_leap, x_leap_back]
    for device in partners:
        pl.semaphore_signal(barrier, inc=1, device_id=device, device_id_type=MESH)
    pl.semaphore_wait(barrier, len(partners))

    def share(w, mat, owner):
        ref = piece(w, mat, owner)
        remote(ref, ref, sib_send.at[w * 3 + mat], sib_recv.at[w * 3 + mat], sibling).start()

    def pass_on(w, mat, owner, n):
        ref = piece(w, mat, owner)
        remote(ref, ref, y_send.at[w * 3 + mat], y_recv.at[n], y_next).start()

    def own(w, mat):
        if w == 2:
            ref = piece(2, mat, f)
            remote(ref, ref, fin_send.at[mat], fin_recv.at[mat], x_leap).wait_recv()
        pass_on(w, mat, f, w * per_set + mat)
        share(w, mat, f)

    def y_tick(n):
        w = n // per_set
        r = n % per_set
        step = r // 3
        owner = CORES * ((y - d * (step + 1) + CORES * n_y) % n_y) + c

        def arrived(mat):
            ref = piece(w, mat, owner)
            remote(ref, ref, y_send.at[w * 3 + mat], y_recv.at[n], y_next).wait_recv()

            @pl.when(step < y_hops - 1)
            def _():
                pass_on(w, mat, owner, n + 3)

            for done in range(2):
                @pl.when((step == y_hops - 1) & (w == done))
                def _():
                    own(done + 1, mat)

            share(w, mat, owner)

        for mat in range(3):
            @pl.when((n < 3 * per_set) & (r % 3 == mat))
            def _():
                arrived(mat)

    def wait_siblings(w):
        for mat in range(3):
            ref = many(w, mat, n_y)
            remote(ref, ref, sib_send.at[w * 3 + mat], sib_recv.at[w * 3 + mat], sibling).wait_recv()

    for mat in range(3):
        loads[1 + mat].wait()
        own(0, mat)

    loads[0].wait()
    for m in range(SUBS):
        part = pl.ds(m * sub, sub)
        x1[0, part, :] = rms_norm(st[part, :].astype(F32), gains[0])
        remote(tok(x1, 0, m), tok(x1, 1, m), ag1_send, ag1_recv.at[m], x_next).start()

    relay = (rg, ru, rd)
    for mat in range(3):
        loads[4 + mat].wait()
        remote(piece(1, mat, f), relay[mat], rel_send.at[mat], rel_recv.at[mat], x_leap).start()

    def ag1_tick(k, m, last):
        remote(tok(x1, k, m), tok(x1, k, m), ag1_send, ag1_recv.at[(k - 1) * SUBS + m], x_next).wait_recv()
        if not last:
            remote(tok(x1, k, m), tok(x1, k + 1, m), ag1_send, ag1_recv.at[k * SUBS + m], x_next).start()

    relay_at = max(1, n_y // 2 - 1)

    pause = 3 * leap

    def extra(n, count):
        def body(i, carry):
            y_tick(n + i)
            return carry
        lax.fori_loop(0, count, body, 0)

    def gather_first(k, n):
        @pl.when(k == relay_at)
        def _():
            for mat in range(3):
                remote(relay[mat], relay[mat], rel_send.at[mat], rel_recv.at[mat], x_leap).wait_recv()
                remote(relay[mat], piece(2, mat, f), fin_send.at[mat], fin_recv.at[mat], x_leap).start()

        late = (k == 2) | (k == relay_at + 1)

        @pl.when(late)
        def _():
            extra(n, pause)

        n = n + jnp.where(late, pause, 0)
        for m in range(SUBS):
            ag1_tick(k, m, False)
            y_tick(n + m)
        return n + SUBS

    ticks = lax.fori_loop(1, hops - 1, gather_first, 0)
    wait_siblings(0)

    def hidden_part(tokens, w, lo, width):
        gate = jnp.dot(tokens, wg[w, :, lo:lo + width], preferred_element_type=F32)
        up = jnp.dot(tokens, wu[w, :, lo:lo + width], preferred_element_type=F32)
        return ((gate / (1.0 + jnp.exp(-gate))) * up).astype(BF16)

    ff = wg.shape[2]
    feats = wd.shape[2]

    def first_quarter(k, m):
        if m < 2:
            width = ff // 2
            lo = m * width
            hid[0, :, lo:lo + width] = hidden_part(x1[k], 0, lo, width)
        else:
            width = feats // 2
            lo = (m - 2) * width
            p1[k, :, lo:lo + width] = jnp.dot(
                hid[0], wd[0, :, lo:lo + width], preferred_element_type=F32
            ).astype(BF16)

    def rs1_copy(src, k, m):
        return remote(src, tok(s1, k - 1, m), rs1_send, rs1_recv.at[(k - 1) * SUBS + m], x_next)

    def reduce_first(j, n):
        for m in range(SUBS):
            @pl.when(j == 0)
            def _():
                ag1_tick(hops - 1, m, False)

            @pl.when(j == 1)
            def _():
                ag1_tick(hops, m, True)
                rs1_copy(tok(p1, 1, m), 1, m).start()

            @pl.when(j >= 2)
            def _():
                part = pl.ds(m * sub, sub)
                rs1_copy(tok(s1, j - 2, m), j - 1, m).wait_recv()
                s1[j - 2, part, :] = (
                    s1[j - 2, part, :].astype(F32) + p1[j, part, :].astype(F32)
                ).astype(BF16)
                rs1_copy(tok(s1, j - 2, m), j, m).start()

            y_tick(n + m)
            first_quarter((j + 1) % n_x, m)
        return n + SUBS

    ticks = lax.fori_loop(0, n_x, reduce_first, ticks)

    for m in range(SUBS):
        part = pl.ds(m * sub, sub)
        rs1_copy(tok(s1, hops - 1, m), hops, m).wait_recv()
        total = s1[hops - 1, part, :].astype(F32) + p1[0, part, :].astype(F32)
        middle = (st[part, :].astype(F32) + 0.5 * total).astype(BF16)
        mid[part, :] = middle
        x2[0, part, :] = rms_norm(middle.astype(F32), gains[1])
        remote(tok(x2, 0, m), tok(x2, 1, m), ag2_send, ag2_recv.at[m], x_next).start()

    def rest(n, carry):
        y_tick(n)
        return carry

    lax.fori_loop(ticks, 3 * per_set, rest, 0)
    wait_siblings(1)
    wait_siblings(2)

    def second_quarter(k, m, lo_row, count):
        tokens = pl.ds(lo_row, count)
        if m < 2:
            width = ff // 2
            for lo in (0, width):
                hid[m, tokens, lo:lo + width] = hidden_part(x2[k, tokens, :], 1 + m, lo, width)
        else:
            width = feats // 2
            lo = (m - 2) * width
            p2[k, tokens, lo:lo + width] = (
                jnp.dot(hid[0, tokens, :], wd[1, :, lo:lo + width], preferred_element_type=F32)
                + jnp.dot(hid[1, tokens, :], wd[2, :, lo:lo + width], preferred_element_type=F32)
            ).astype(BF16)

    def ag2_arrival(k, m):
        remote(tok(x2, k, m), tok(x2, k, m), ag2_send, ag2_recv.at[(k - 1) * SUBS + m], x_next).wait_recv()

    def gather_second(k, carry):
        for m in range(SUBS):
            @pl.when(k < wide - 1)
            def _():
                ag2_arrival(k, m)
                remote(tok(x2, k, m), tok(x2, k + 1, m), ag2_send, ag2_recv.at[k * SUBS + m], x_next).start()

            if m < 2:
                second_quarter(k - 1, 2 * m, 0, rows)
                second_quarter(k - 1, 2 * m + 1, 0, rows)
        return carry

    lax.fori_loop(1, wide, gather_second, 0)

    def rs2_copy(src, k, m):
        return remote(src, tok(s2, k - 1, m), rs2_send, rs2_recv.at[(k - 1) * SUBS + m], x_prev)

    half = rows // 2

    def last_block(h, carry):
        for m in range(SUBS // 2):
            ag2_arrival(wide - 1, h * (SUBS // 2) + m)
        for q in range(4):
            second_quarter(wide - 1, q, pl.multiple_of(h * half, half), half)
        for m in range(SUBS // 2):
            rs2_copy(tok(p2, wide - 1, h * (SUBS // 2) + m), wide - 1, h * (SUBS // 2) + m).start()
        return carry

    lax.fori_loop(0, 2, last_block, 0)

    for k in range(wide - 2, 0, -1):
        for m in range(SUBS):
            part = pl.ds(m * sub, sub)
            rs2_copy(tok(s2, k, m), k + 1, m).wait_recv()
            s2[k, part, :] = (
                s2[k, part, :].astype(F32) + p2[k, part, :].astype(F32)
            ).astype(BF16)
            rs2_copy(tok(s2, k, m), k, m).start()

    for m in range(SUBS):
        part = pl.ds(m * sub, sub)
        rs2_copy(tok(s2, 0, m), 1, m).wait_recv()
        total = s2[0, part, :].astype(F32) + p2[0, part, :].astype(F32)
        out[part, :] = (mid[part, :].astype(F32) + 0.5 * total).astype(BF16)

    def sent(ref, sem):
        remote(ref, ref, sem, rel_recv.at[0], sibling).wait_send()

    sent(x1.at[pl.ds(0, hops)], ag1_send)
    sent(s1, rs1_send)
    sent(x2.at[pl.ds(0, wide - 1)], ag2_send)
    sent(s2, rs2_send)
    for mat in range(3):
        sent(relay[mat], rel_send.at[mat])
        sent(relay[mat], fin_send.at[mat])
        for w in range(3):
            sent(many(w, mat, y_hops), y_send.at[w * 3 + mat])
            sent(many(w, mat, n_y), sib_send.at[w * 3 + mat])


def solution(mesh):
    n_x = mesh.shape["tp"]
    n_y = mesh.shape["fs"] // CORES

    def local(stream, gain1, g1, u1, d1, gain2, g2, u2, d2):
        rows, feats = stream.shape
        shard, ff = g1.shape
        wide = n_x // 2
        any_spec = pl.BlockSpec(memory_space=pl.ANY)
        vmem_spec = pl.BlockSpec(memory_space=pltpu.VMEM)
        dma = pltpu.SemaphoreType.DMA
        y_count = 9 * (n_y - 1)
        return pl.pallas_call(
            functools.partial(kernel, n_x, n_y),
            out_shape=jax.ShapeDtypeStruct((rows, feats), BF16),
            in_specs=[any_spec, vmem_spec, any_spec, any_spec, any_spec,
                      vmem_spec, any_spec, any_spec, any_spec],
            out_specs=vmem_spec,
            scratch_shapes=[
                pltpu.VMEM((3, feats, ff), BF16),
                pltpu.VMEM((3, feats, ff), BF16),
                pltpu.VMEM((3, ff, feats), BF16),
                pltpu.VMEM((rows, feats), BF16),
                pltpu.VMEM((n_x, rows, feats), BF16),
                pltpu.VMEM((n_x, rows, feats), BF16),
                pltpu.VMEM((n_x - 1, rows, feats), BF16),
                pltpu.VMEM((rows, feats), BF16),
                pltpu.VMEM((wide, rows, feats), BF16),
                pltpu.VMEM((wide, rows, feats), BF16),
                pltpu.VMEM((wide - 1, rows, feats), BF16),
                pltpu.VMEM((shard, ff), BF16),
                pltpu.VMEM((shard, ff), BF16),
                pltpu.VMEM((ff, shard), BF16),
                pltpu.VMEM((2, rows, ff), BF16),
                pltpu.VMEM((2, 1, feats), F32),
                dma((7,)),
                dma(((n_x - 1) * SUBS,)),
                dma(((n_x - 1) * SUBS,)),
                dma(((wide - 1) * SUBS,)),
                dma(((wide - 1) * SUBS,)),
                dma((y_count,)),
                dma((9,)),
                dma((3,)),
                dma((3,)),
                dma,
                dma,
                dma,
                dma,
                dma((9,)),
                dma((9,)),
                dma((3,)),
                dma((3,)),
            ],
            compiler_params=pltpu.CompilerParams(
                collective_id=0, has_side_effects=True, vmem_limit_bytes=60 * 1024 * 1024
            ),
        )(stream, gain1.reshape(-1, LANES), g1, u1, d1, gain2.reshape(-1, LANES), g2, u2, d2)

    tokens = P(("grp", "fs", "tp"), None)
    rows_split, cols_split = P("fs", "tp"), P("tp", "fs")
    in_specs = (
        tokens,
        P(), rows_split, rows_split, cols_split,
        P(), rows_split, rows_split, cols_split,
    )
    return jax.shard_map(local, mesh=mesh, in_specs=in_specs, out_specs=tokens, check_vma=False)
```

```python
import functools

import jax
import jax.numpy as jnp
from jax import lax
from jax.experimental import pallas as pl
from jax.experimental.pallas import tpu as pltpu
from jax.sharding import PartitionSpec as P

MESH = pl.DeviceIdType.MESH
F32 = jnp.float32
BF16 = jnp.bfloat16
SUBS = 4
CORES = 2
LANES = 128


def rms_norm(rows_f, gain):
    scale = lax.rsqrt(jnp.mean(rows_f * rows_f, axis=-1, keepdims=True) + 1e-06)
    return (rows_f * scale * gain).astype(BF16)


def kernel(
    n_x, n_y,
    stream, gain1, g1, u1, d1, gain2, g2, u2, d2,
    out,
    wg, wu, wd, st, x1, p1, s1, mid, x2, p2, s2, rg, ru, rd, hid, gains,
    load_sem, ag1_recv, rs1_recv, ag2_recv, rs2_recv, y_recv, sib_recv, rel_recv, fin_recv,
    ag1_send, rs1_send, ag2_send, rs2_send, y_send, sib_send, rel_send, fin_send, turn,
):
    x = lax.axis_index("tp")
    f = lax.axis_index("fs")
    y = f // CORES
    c = f % CORES
    d = 1 - 2 * c
    hops = n_x - 1
    wide = n_x // 2
    leap = n_x // 4
    rows = st.shape[0]
    sub = rows // SUBS
    shard = g1.shape[0]
    y_hops = n_y - 1
    per_set = 3 * y_hops

    x_next = {"tp": (x + d + n_x) % n_x}
    x_prev = {"tp": (x - d + n_x) % n_x}
    x_leap = {"tp": (x + leap * d + n_x) % n_x}
    x_leap_back = {"tp": (x - leap * d + n_x) % n_x}
    y_next = {"fs": CORES * ((y + d + n_y) % n_y) + c}
    y_prev = {"fs": CORES * ((y - d + n_y) % n_y) + c}
    sibling = {"fs": CORES * y + 1 - c}

    def remote(src, dst, send, recv, device):
        return pltpu.make_async_remote_copy(
            src_ref=src, dst_ref=dst, send_sem=send, recv_sem=recv,
            device_id=device, device_id_type=MESH,
        )

    def piece(w, mat, owner):
        span = pl.ds(pl.multiple_of(owner * shard, shard), shard)
        if mat == 0:
            return wg.at[w, span, :]
        if mat == 1:
            return wu.at[w, span, :]
        return wd.at[w, :, span]

    def many(w, mat, count):
        span = pl.ds(0, count * shard)
        if mat == 0:
            return wg.at[w, span, :]
        if mat == 1:
            return wu.at[w, span, :]
        return wd.at[w, :, span]

    def tok(ref, k, m):
        return ref.at[k, pl.ds(pl.multiple_of(m * sub, sub), sub), :]

    barrier = pltpu.get_barrier_semaphore()
    partners = [x_next, x_prev, y_next, y_prev, sibling]
    if leap > 1:
        partners += [x_leap, x_leap_back]
    for device in partners:
        pl.semaphore_signal(barrier, inc=1, device_id=device, device_id_type=MESH)
    loads = [pltpu.make_async_copy(stream, st, load_sem.at[0])]
    for i, (src, w, mat) in enumerate(
        ((g1, 0, 0), (u1, 0, 1), (d1, 0, 2), (g2, 1, 0), (u2, 1, 1), (d2, 1, 2))
    ):
        loads.append(pltpu.make_async_copy(src, piece(w, mat, f), load_sem.at[1 + i]))
    for copy in loads:
        copy.start()
    for i, gain in enumerate((gain1, gain2)):
        for j in range(gain.shape[0]):
            gains[i, :, j * LANES:(j + 1) * LANES] = gain[j:j + 1, :].astype(F32)
    pl.semaphore_wait(barrier, len(partners))

    def share(w, mat, owner):
        ref = piece(w, mat, owner)
        remote(ref, ref, sib_send.at[w * 3 + mat], sib_recv.at[w * 3 + mat], sibling).start()

    def pass_on(w, mat, owner, n):
        ref = piece(w, mat, owner)
        remote(ref, ref, y_send.at[w * 3 + mat], y_recv.at[n], y_next).start()

    def own(w, mat):
        if w == 2:
            ref = piece(2, mat, f)
            remote(ref, ref, fin_send.at[mat], fin_recv.at[mat], x_leap).wait_recv()
        pass_on(w, mat, f, w * per_set + mat)
        share(w, mat, f)

    def y_tick(n):
        w = n // per_set
        r = n % per_set
        step = r // 3
        owner = CORES * ((y - d * (step + 1) + CORES * n_y) % n_y) + c

        def arrived(mat):
            ref = piece(w, mat, owner)
            remote(ref, ref, y_send.at[w * 3 + mat], y_recv.at[n], y_next).wait_recv()

            @pl.when(step < y_hops - 1)
            def _():
                pass_on(w, mat, owner, n + 3)

            for done in range(2):
                @pl.when((step == y_hops - 1) & (w == done))
                def _():
                    own(done + 1, mat)

            share(w, mat, owner)

        for mat in range(3):
            @pl.when((n < 3 * per_set) & (r % 3 == mat))
            def _():
                arrived(mat)

    def wait_siblings(w):
        for mat in range(3):
            ref = many(w, mat, n_y)
            remote(ref, ref, sib_send.at[w * 3 + mat], sib_recv.at[w * 3 + mat], sibling).wait_recv()

    for mat in range(3):
        loads[1 + mat].wait()
        own(0, mat)

    loads[0].wait()
    for m in range(SUBS):
        part = pl.ds(m * sub, sub)
        x1[0, part, :] = rms_norm(st[part, :].astype(F32), gains[0])
        remote(tok(x1, 0, m), tok(x1, 1, m), ag1_send, ag1_recv.at[m], x_next).start()

    relay = (rg, ru, rd)
    for mat in range(3):
        loads[4 + mat].wait()
        remote(piece(1, mat, f), relay[mat], rel_send.at[mat], rel_recv.at[mat], x_leap).start()

    def ag1_tick(k, m, last):
        remote(tok(x1, k, m), tok(x1, k, m), ag1_send, ag1_recv.at[(k - 1) * SUBS + m], x_next).wait_recv()
        if not last:
            remote(tok(x1, k, m), tok(x1, k + 1, m), ag1_send, ag1_recv.at[k * SUBS + m], x_next).start()

    relay_at = max(1, n_y // 2 - 1)

    pause = 3 * leap - 1

    def extra(n, count):
        def body(i, carry):
            y_tick(n + i)
            return carry
        lax.fori_loop(0, count, body, 0)

    def gather_first(k, n):
        @pl.when(k == relay_at)
        def _():
            for mat in range(3):
                remote(relay[mat], relay[mat], rel_send.at[mat], rel_recv.at[mat], x_leap).wait_recv()
                remote(relay[mat], piece(2, mat, f), fin_send.at[mat], fin_recv.at[mat], x_leap).start()

        late = (k == 2) | (k == relay_at + 1)

        @pl.when(late)
        def _():
            extra(n, pause)

        n = n + jnp.where(late, pause, 0)
        for m in range(SUBS):
            ag1_tick(k, m, False)

            @pl.when(k > 1)
            def _():
                y_tick(n + m)
        return n + jnp.where(k > 1, SUBS, 0)

    def rest(n, carry):
        y_tick(n)
        return carry

    ticks = lax.fori_loop(1, hops - 1, gather_first, 0)
    lax.fori_loop(ticks, per_set, rest, 0)
    ticks = jnp.maximum(ticks, per_set)
    wait_siblings(0)

    def hidden_part(tokens, w, lo, width):
        gate = jnp.dot(tokens, wg[w, :, lo:lo + width], preferred_element_type=F32)
        up = jnp.dot(tokens, wu[w, :, lo:lo + width], preferred_element_type=F32)
        return ((gate / (1.0 + jnp.exp(-gate))) * up).astype(BF16)

    ff = wg.shape[2]
    feats = wd.shape[2]

    def first_quarter(k, m):
        if m < 2:
            width = ff // 2
            lo = m * width
            hid[0, :, lo:lo + width] = hidden_part(x1[k], 0, lo, width)
        else:
            width = feats // 2
            lo = (m - 2) * width
            p1[k, :, lo:lo + width] = jnp.dot(
                hid[0], wd[0, :, lo:lo + width], preferred_element_type=F32
            ).astype(BF16)

    def rs1_copy(src, k, m):
        return remote(src, tok(s1, k - 1, m), rs1_send, rs1_recv.at[(k - 1) * SUBS + m], x_next)

    def reduce_first(j, n):
        for m in range(SUBS):
            @pl.when(j == 0)
            def _():
                ag1_tick(hops - 1, m, False)

            @pl.when(j == 1)
            def _():
                ag1_tick(hops, m, True)
                rs1_copy(tok(p1, 1, m), 1, m).start()

            @pl.when(j >= 2)
            def _():
                part = pl.ds(m * sub, sub)
                rs1_copy(tok(s1, j - 2, m), j - 1, m).wait_recv()
                s1[j - 2, part, :] = (
                    s1[j - 2, part, :].astype(F32) + p1[j, part, :].astype(F32)
                ).astype(BF16)
                rs1_copy(tok(s1, j - 2, m), j, m).start()

            y_tick(n + m)
            first_quarter((j + 1) % n_x, m)
        return n + SUBS

    ticks = lax.fori_loop(0, n_x, reduce_first, ticks)

    for m in range(SUBS):
        part = pl.ds(m * sub, sub)
        rs1_copy(tok(s1, hops - 1, m), hops, m).wait_recv()
        total = s1[hops - 1, part, :].astype(F32) + p1[0, part, :].astype(F32)
        middle = (st[part, :].astype(F32) + 0.5 * total).astype(BF16)
        mid[part, :] = middle
        x2[0, part, :] = rms_norm(middle.astype(F32), gains[1])
        remote(tok(x2, 0, m), tok(x2, 1, m), ag2_send, ag2_recv.at[m], x_next).start()
        y_tick(ticks + m)

    def ag2_arrival(t):
        k, m = 1 + t // SUBS, t % SUBS
        remote(tok(x2, k, m), tok(x2, k, m), ag2_send, ag2_recv.at[t], x_next).wait_recv()

    passes = (wide - 2) * SUBS

    def hand_over():
        pl.semaphore_signal(turn, inc=1, device_id=sibling, device_id_type=MESH)

    def ag2_tick(t):
        @pl.when(t < passes)
        def _():
            ag2_arrival(t)
            k, m = 1 + t // SUBS, t % SUBS
            remote(tok(x2, k, m), tok(x2, k + 1, m), ag2_send, ag2_recv.at[t + SUBS], x_next).start()

        @pl.when(t == passes - 1)
        def _():
            hand_over()

    for t in range(SUBS):
        ag2_tick(t)
    if not passes:
        hand_over()

    lax.fori_loop(ticks + SUBS, 3 * per_set, rest, 0)
    wait_siblings(1)
    wait_siblings(2)

    def second_quarter(k, m, lo_row, count):
        tokens = pl.ds(lo_row, count)
        if m < 2:
            width = ff // 2
            for lo in (0, width):
                hid[m, tokens, lo:lo + width] = hidden_part(x2[k, tokens, :], 1 + m, lo, width)
        else:
            width = feats // 2
            lo = (m - 2) * width
            p2[k, tokens, lo:lo + width] = (
                jnp.dot(hid[0, tokens, :], wd[1, :, lo:lo + width], preferred_element_type=F32)
                + jnp.dot(hid[1, tokens, :], wd[2, :, lo:lo + width], preferred_element_type=F32)
            ).astype(BF16)

    def gather_second(k, carry):
        for m in range(2):
            ag2_tick(SUBS + 2 * k + m)
            second_quarter(k, 2 * m, 0, rows)
            second_quarter(k, 2 * m + 1, 0, rows)
        return carry

    lax.fori_loop(0, wide - 1, gather_second, 0)

    def rs2_copy(src, k, m):
        return remote(src, tok(s2, k - 1, m), rs2_send, rs2_recv.at[(k - 1) * SUBS + m], x_prev)

    half = rows // 2

    def last_block(h, carry):
        for m in range(SUBS // 2):
            ag2_arrival(passes + h * (SUBS // 2) + m)
        for q in range(4):
            second_quarter(wide - 1, q, pl.multiple_of(h * half, half), half)

        @pl.when(h == 0)
        def _():
            pl.semaphore_wait(turn, 1)

        for m in range(SUBS // 2):
            rs2_copy(tok(p2, wide - 1, h * (SUBS // 2) + m), wide - 1, h * (SUBS // 2) + m).start()
        return carry

    lax.fori_loop(0, 2, last_block, 0)

    for k in range(wide - 2, 0, -1):
        for m in range(SUBS):
            part = pl.ds(m * sub, sub)
            rs2_copy(tok(s2, k, m), k + 1, m).wait_recv()
            s2[k, part, :] = (
                s2[k, part, :].astype(F32) + p2[k, part, :].astype(F32)
            ).astype(BF16)
            rs2_copy(tok(s2, k, m), k, m).start()

    for m in range(SUBS):
        part = pl.ds(m * sub, sub)
        rs2_copy(tok(s2, 0, m), 1, m).wait_recv()
        total = s2[0, part, :].astype(F32) + p2[0, part, :].astype(F32)
        out[part, :] = (mid[part, :].astype(F32) + 0.5 * total).astype(BF16)

    def sent(ref, sem):
        remote(ref, ref, sem, rel_recv.at[0], sibling).wait_send()

    sent(x1.at[pl.ds(0, hops)], ag1_send)
    sent(s1, rs1_send)
    sent(x2.at[pl.ds(0, wide - 1)], ag2_send)
    sent(s2, rs2_send)
    for mat in range(3):
        sent(relay[mat], rel_send.at[mat])
        sent(relay[mat], fin_send.at[mat])
        for w in range(3):
            sent(many(w, mat, y_hops), y_send.at[w * 3 + mat])
            sent(many(w, mat, n_y), sib_send.at[w * 3 + mat])


def solution(mesh):
    n_x = mesh.shape["tp"]
    n_y = mesh.shape["fs"] // CORES

    def local(stream, gain1, g1, u1, d1, gain2, g2, u2, d2):
        rows, feats = stream.shape
        shard, ff = g1.shape
        wide = n_x // 2
        any_spec = pl.BlockSpec(memory_space=pl.ANY)
        vmem_spec = pl.BlockSpec(memory_space=pltpu.VMEM)
        dma = pltpu.SemaphoreType.DMA
        y_count = 9 * (n_y - 1)
        return pl.pallas_call(
            functools.partial(kernel, n_x, n_y),
            out_shape=pltpu.VMEM((rows, feats), BF16),
            in_specs=[any_spec, vmem_spec, any_spec, any_spec, any_spec,
                      vmem_spec, any_spec, any_spec, any_spec],
            out_specs=vmem_spec,
            scratch_shapes=[
                pltpu.VMEM((3, feats, ff), BF16),
                pltpu.VMEM((3, feats, ff), BF16),
                pltpu.VMEM((3, ff, feats), BF16),
                pltpu.VMEM((rows, feats), BF16),
                pltpu.VMEM((n_x, rows, feats), BF16),
                pltpu.VMEM((n_x, rows, feats), BF16),
                pltpu.VMEM((n_x - 1, rows, feats), BF16),
                pltpu.VMEM((rows, feats), BF16),
                pltpu.VMEM((wide, rows, feats), BF16),
                pltpu.VMEM((wide, rows, feats), BF16),
                pltpu.VMEM((wide - 1, rows, feats), BF16),
                pltpu.VMEM((shard, ff), BF16),
                pltpu.VMEM((shard, ff), BF16),
                pltpu.VMEM((ff, shard), BF16),
                pltpu.VMEM((2, rows, ff), BF16),
                pltpu.VMEM((2, 1, feats), F32),
                dma((7,)),
                dma(((n_x - 1) * SUBS,)),
                dma(((n_x - 1) * SUBS,)),
                dma(((wide - 1) * SUBS,)),
                dma(((wide - 1) * SUBS,)),
                dma((y_count,)),
                dma((9,)),
                dma((3,)),
                dma((3,)),
                dma,
                dma,
                dma,
                dma,
                dma((9,)),
                dma((9,)),
                dma((3,)),
                dma((3,)),
                pltpu.SemaphoreType.REGULAR,
            ],
            compiler_params=pltpu.CompilerParams(
                collective_id=0, has_side_effects=True, vmem_limit_bytes=60 * 1024 * 1024
            ),
        )(stream, gain1.reshape(-1, LANES), g1, u1, d1, gain2.reshape(-1, LANES), g2, u2, d2)

    tokens = P(("grp", "fs", "tp"), None)
    rows_split, cols_split = P("fs", "tp"), P("tp", "fs")
    in_specs = (
        tokens,
        P(), rows_split, rows_split, cols_split,
        P(), rows_split, rows_split, cols_split,
    )
    return jax.shard_map(local, mesh=mesh, in_specs=in_specs, out_specs=tokens, check_vma=False)
```

```python
import functools

import jax
import jax.numpy as jnp
from jax import lax
from jax.experimental import pallas as pl
from jax.experimental.pallas import tpu as pltpu
from jax.sharding import PartitionSpec as P

MESH = pl.DeviceIdType.MESH
F32 = jnp.float32
BF16 = jnp.bfloat16
SUBS = 4
CORES = 2
LANES = 128


def rms_norm(rows_f, gain):
    scale = lax.rsqrt(jnp.mean(rows_f * rows_f, axis=-1, keepdims=True) + 1e-06)
    return (rows_f * scale * gain).astype(BF16)


def kernel(
    n_x, n_y,
    stream, gain1, g1, u1, d1, gain2, g2, u2, d2,
    out,
    wg, wu, wd, st, x1, p1, s1, mid, x2, p2, s2, rg, ru, rd, hid, gains,
    load_sem, ag1_recv, rs1_recv, ag2_recv, rs2_recv, y_recv, sib_recv, rel_recv, fin_recv,
    ag1_send, rs1_send, ag2_send, rs2_send, y_send, sib_send, rel_send, fin_send, both_in,
):
    x = lax.axis_index("tp")
    f = lax.axis_index("fs")
    y = f // CORES
    c = f % CORES
    d = 1 - 2 * c
    hops = n_x - 1
    wide = n_x // 2
    leap = n_x // 4
    rows = st.shape[0]
    sub = rows // SUBS
    shard = g1.shape[0]
    y_hops = n_y - 1

    x_near = ({"tp": (x + 1) % n_x}, {"tp": (x - 1 + n_x) % n_x})
    x_leap = {"tp": (x + leap * d + n_x) % n_x}
    x_leap_back = {"tp": (x - leap * d + n_x) % n_x}
    y_next = {"fs": CORES * ((y + d + n_y) % n_y) + c}
    y_prev = {"fs": CORES * ((y - d + n_y) % n_y) + c}
    sibling = {"fs": CORES * y + 1 - c}

    def remote(src, dst, send, recv, device):
        return pltpu.make_async_remote_copy(
            src_ref=src, dst_ref=dst, send_sem=send, recv_sem=recv,
            device_id=device, device_id_type=MESH,
        )

    def piece(w, mat, owner):
        span = pl.ds(pl.multiple_of(owner * shard, shard), shard)
        if mat == 0:
            return wg.at[w, span, :]
        if mat == 1:
            return wu.at[w, span, :]
        return wd.at[w, :, span]

    def many(w, mat, count):
        span = pl.ds(0, count * shard)
        if mat == 0:
            return wg.at[w, span, :]
        if mat == 1:
            return wu.at[w, span, :]
        return wd.at[w, :, span]

    bit = sub // 2

    class Halves:
        def __init__(self, src, src_k, dst, dst_k, m, send, recv, slot, back=False):
            self.args = src, src_k, dst, dst_k, m, send, recv, slot, back

        def start(self):
            src, src_k, dst, dst_k, m, send, recv, slot, back = self.args
            for way in range(2):
                span = pl.ds(pl.multiple_of(m * sub, sub) + way * bit, bit)
                remote(
                    src.at[src_k, span, :], dst.at[dst_k, span, :], send,
                    recv.at[slot], x_near[1 - way if back else way],
                ).start()

        def wait_recv(self):
            _, _, dst, dst_k, m, send, recv, slot, _ = self.args
            whole = dst.at[dst_k, pl.ds(pl.multiple_of(m * sub, sub), sub), :]
            remote(whole, whole, send, recv.at[slot], x_near[0]).wait_recv()

    def relay_on(came, goes):
        came.wait_recv()
        goes.start()

    barrier = pltpu.get_barrier_semaphore()
    partners = [x_near[0], x_near[1], y_next, y_prev]
    if leap > 1:
        partners += [x_leap, x_leap_back]
    for device in partners:
        pl.semaphore_signal(barrier, inc=1, device_id=device, device_id_type=MESH)

    @pl.when(c == 1)
    def _():
        witness = {"fs": CORES * y, "tp": (x + 1) % n_x}
        pl.semaphore_signal(barrier, inc=1, device_id=witness, device_id_type=MESH)

    loads = [pltpu.make_async_copy(stream, st, load_sem.at[0])]
    for i, (src, w, mat) in enumerate(
        ((g1, 0, 0), (u1, 0, 1), (d1, 0, 2), (g2, 1, 0), (u2, 1, 1), (d2, 1, 2))
    ):
        loads.append(pltpu.make_async_copy(src, piece(w, mat, f), load_sem.at[1 + i]))
    for copy in loads:
        copy.start()
    for i, gain in enumerate((gain1, gain2)):
        for j in range(gain.shape[0]):
            gains[i, :, j * LANES:(j + 1) * LANES] = gain[j:j + 1, :].astype(F32)
    pl.semaphore_wait(barrier, len(partners) + 1 - c)

    @pl.when(c == 0)
    def _():
        for core in range(CORES):
            device = {"fs": CORES * y + core, "tp": (x - 1 + n_x) % n_x}
            pl.semaphore_signal(both_in, inc=1, device_id=device, device_id_type=MESH)

    head = 4
    first_ticks = head * y_hops
    all_ticks = 9 * y_hops

    def share(w, mat, owner):
        ref = piece(w, mat, owner)
        remote(ref, ref, sib_send.at[mat], sib_recv.at[w * 3 + mat], sibling).start()

    def pass_on(w, mat, owner, n):
        ref = piece(w, mat, owner)
        remote(ref, ref, y_send.at[mat], y_recv.at[n], y_next).start()

    def share_item(i):
        owner = CORES * ((y - d * (i // head) + CORES * n_y) % n_y) + c
        item = i % head
        for mat in range(3):
            @pl.when(item % 3 == mat)
            def _():
                share(item // 3, mat, owner)

    def own(item):
        w, mat = item // 3, item % 3
        if w == 2:
            ref = piece(2, mat, f)
            remote(ref, ref, fin_send.at[mat], fin_recv.at[mat], x_leap).wait_recv()
        if item < head:
            pass_on(w, mat, f, item)
        else:
            pass_on(w, mat, f, first_ticks + item - head)
            share(w, mat, f)

    def y_tick(n, sharing=True):
        late = n >= first_ticks
        r = n - jnp.where(late, first_ticks, 0)
        step = jnp.where(late, r // (9 - head), r // head)
        size = jnp.where(late, 9 - head, head)
        item = r - step * size + jnp.where(late, head, 0)
        w = item // 3
        owner = CORES * ((y - d * (step + 1) + CORES * n_y) % n_y) + c

        def arrived(mat):
            ref = piece(w, mat, owner)
            remote(ref, ref, y_send.at[mat], y_recv.at[n], y_next).wait_recv()

            @pl.when(step < y_hops - 1)
            def _():
                pass_on(w, mat, owner, n + size)

            if sharing is True:
                share(w, mat, owner)
            else:
                @pl.when(sharing)
                def _():
                    share(w, mat, owner)

        for mat in range(3):
            @pl.when((n < all_ticks) & (item % 3 == mat))
            def _():
                arrived(mat)

        for item_own in range(head, 9):
            @pl.when((n < first_ticks) & (step == y_hops - 1) & (item == min(item_own - head, head - 1)))
            def _():
                own(item_own)

    def wait_siblings(w):
        for mat in range(3):
            ref = many(w, mat, n_y)
            remote(ref, ref, sib_send.at[mat], sib_recv.at[w * 3 + mat], sibling).wait_recv()

    def ag1_copy(k, m):
        return Halves(x1, k, x1, k + 1, m, ag1_send, ag1_recv, k * SUBS + m)

    loads[0].wait()
    for m in range(SUBS):
        part = pl.ds(m * sub, sub)
        x1[0, part, :] = rms_norm(st[part, :].astype(F32), gains[0])
        ag1_copy(0, m).start()
        if m == 0:
            for item in range(head):
                loads[1 + item].wait()
                own(item)

    relay = (rg, ru, rd)
    for mat in range(3):
        if mat:
            loads[4 + mat].wait()
        remote(piece(1, mat, f), relay[mat], rel_send.at[mat], rel_recv.at[mat], x_leap).start()

    def ag1_tick(k, m, last):
        if last:
            ag1_copy(k - 1, m).wait_recv()
        else:
            relay_on(ag1_copy(k - 1, m), ag1_copy(k, m))

    relay_at = max(1, n_y // 2 - 1)
    share_at = max(1, min(relay_at + 1, hops - 2))

    pause = 3 * leap

    def extra(n, count, sharing):
        def body(i, carry):
            y_tick(n + i, sharing)
            return carry
        lax.fori_loop(0, count, body, 0)

    def gather_first(k, n):
        @pl.when(k == relay_at)
        def _():
            for mat in range(3):
                remote(relay[mat], relay[mat], rel_send.at[mat], rel_recv.at[mat], x_leap).wait_recv()
                remote(relay[mat], piece(2, mat, f), fin_send.at[mat], fin_recv.at[mat], x_leap).start()

        @pl.when(k == share_at)
        def _():
            pl.semaphore_wait(both_in, 1)

            def body(i, carry):
                share_item(i)
                return carry
            lax.fori_loop(0, jnp.maximum(n, 0) + head, body, 0)

        late = (k == 2) | (k == relay_at + 1)

        @pl.when(late)
        def _():
            extra(n, pause, k >= share_at)

        n = n + jnp.where(late, pause, 0)
        for m in range(SUBS):
            ag1_tick(k, m, False)

            @pl.when((k > 1) | (m >= SUBS // 2))
            def _():
                y_tick(n + m, k >= share_at)
        return n + SUBS

    def rest(n, carry):
        y_tick(n)
        return carry

    ticks = lax.fori_loop(1, hops - 1, gather_first, -(SUBS // 2))
    lax.fori_loop(ticks, first_ticks, rest, 0)
    ticks = jnp.maximum(ticks, first_ticks)
    wait_siblings(0)

    def hidden_part(tokens, w, lo, width):
        gate = jnp.dot(tokens, wg[w, :, lo:lo + width], preferred_element_type=F32)
        up = jnp.dot(tokens, wu[w, :, lo:lo + width], preferred_element_type=F32)
        return ((gate / (1.0 + jnp.exp(-gate))) * up).astype(BF16)

    ff = wg.shape[2]
    feats = wd.shape[2]

    def first_quarter(k, m):
        if m < 2:
            width = ff // 2
            lo = m * width
            hid[0, :, lo:lo + width] = hidden_part(x1[k], 0, lo, width)
        else:
            width = feats // 2
            lo = (m - 2) * width
            p1[k, :, lo:lo + width] = jnp.dot(
                hid[0], wd[0, :, lo:lo + width], preferred_element_type=F32
            ).astype(BF16)

    def rs1_copy(src, src_k, k, m):
        return Halves(src, src_k, s1, k - 1, m, rs1_send, rs1_recv, (k - 1) * SUBS + m)

    def reduce_first(j, n):
        for m in range(SUBS):
            @pl.when(j == 0)
            def _():
                ag1_tick(hops - 1, m, False)

            @pl.when(j == 1)
            def _():
                ag1_tick(hops, m, True)
                rs1_copy(p1, 1, 1, m).start()

            @pl.when(j >= 2)
            def _():
                part = pl.ds(m * sub, sub)
                rs1_copy(s1, j - 2, j - 1, m).wait_recv()
                s1[j - 2, part, :] = (
                    s1[j - 2, part, :].astype(F32) + p1[j, part, :].astype(F32)
                ).astype(BF16)
                rs1_copy(s1, j - 2, j, m).start()

            y_tick(n + m)
            first_quarter((j + 1) % n_x, m)
        return n + SUBS

    ticks = lax.fori_loop(0, n_x, reduce_first, ticks)

    def ag2_copy(t):
        k, m = t // SUBS, t % SUBS
        return Halves(x2, k, x2, k + 1, m, ag2_send, ag2_recv, t)

    for m in range(SUBS):
        part = pl.ds(m * sub, sub)
        rs1_copy(s1, hops - 1, hops, m).wait_recv()
        total = s1[hops - 1, part, :].astype(F32) + p1[0, part, :].astype(F32)
        middle = (st[part, :].astype(F32) + 0.5 * total).astype(BF16)
        mid[part, :] = middle
        x2[0, part, :] = rms_norm(middle.astype(F32), gains[1])
        ag2_copy(m).start()
        y_tick(ticks + m)

    passes = (wide - 2) * SUBS

    def ag2_tick(t):
        @pl.when(t < passes)
        def _():
            relay_on(ag2_copy(t), ag2_copy(t + SUBS))

    for t in range(SUBS):
        ag2_tick(t)

    lax.fori_loop(ticks + SUBS, all_ticks, rest, 0)
    wait_siblings(1)
    wait_siblings(2)

    def second_quarter(k, m, lo_row, count):
        tokens = pl.ds(lo_row, count)
        if m < 2:
            width = ff // 2
            for lo in (0, width):
                hid[m, tokens, lo:lo + width] = hidden_part(x2[k, tokens, :], 1 + m, lo, width)
        else:
            width = feats // 2
            lo = (m - 2) * width
            p2[k, tokens, lo:lo + width] = (
                jnp.dot(hid[0, tokens, :], wd[1, :, lo:lo + width], preferred_element_type=F32)
                + jnp.dot(hid[1, tokens, :], wd[2, :, lo:lo + width], preferred_element_type=F32)
            ).astype(BF16)

    for t in range(SUBS, passes):
        ag2_tick(t)
    for q in range(4 if wide > 2 else 0):
        second_quarter(wide - 2, q, 0, rows)

    def rs2_copy(src, k, m):
        return Halves(src, k, s2, k - 1, m, rs2_send, rs2_recv, (k - 1) * SUBS + m, back=True)

    half = rows // 2

    def last_block(h, carry):
        for m in range(SUBS // 2):
            ag2_copy(passes + h * (SUBS // 2) + m).wait_recv()
        for q in range(4):
            second_quarter(wide - 1, q, pl.multiple_of(h * half, half), half)
        for m in range(SUBS // 2):
            rs2_copy(p2, wide - 1, h * (SUBS // 2) + m).start()
        return carry

    lax.fori_loop(0, 2, last_block, 0)

    def sent(ref, sem):
        remote(ref, ref, sem, rel_recv.at[0], sibling).wait_send()

    sent(x1.at[pl.ds(0, hops)], ag1_send)
    sent(s1, rs1_send)
    sent(x2.at[pl.ds(0, wide - 1)], ag2_send)
    for mat in range(3):
        sent(relay[mat], rel_send.at[mat])
        sent(relay[mat], fin_send.at[mat])
        sent(many(pl.ds(0, 3), mat, y_hops), y_send.at[mat])
        sent(many(pl.ds(0, 3), mat, n_y), sib_send.at[mat])

    def reduce_second(i, carry):
        k = wide - 2 - i
        for m in range(SUBS):
            part = pl.ds(m * sub, sub)
            rs2_copy(s2, k + 1, m).wait_recv()
            s2[k, part, :] = (
                s2[k, part, :].astype(F32) + p2[k, part, :].astype(F32)
            ).astype(BF16)
            rs2_copy(s2, k, m).start()
            second_quarter(k - 1, m, 0, rows)
        return carry

    if wide > 2:
        lax.fori_loop(0, wide - 2, reduce_second, 0)
    else:
        for q in range(4):
            second_quarter(0, q, 0, rows)

    for m in range(SUBS):
        part = pl.ds(m * sub, sub)
        rs2_copy(s2, 1, m).wait_recv()
        total = s2[0, part, :].astype(F32) + p2[0, part, :].astype(F32)
        out[part, :] = (mid[part, :].astype(F32) + 0.5 * total).astype(BF16)

    sent(s2, rs2_send)


def solution(mesh):
    n_x = mesh.shape["tp"]
    n_y = mesh.shape["fs"] // CORES

    def local(stream, gain1, g1, u1, d1, gain2, g2, u2, d2):
        rows, feats = stream.shape
        shard, ff = g1.shape
        wide = n_x // 2
        any_spec = pl.BlockSpec(memory_space=pl.ANY)
        vmem_spec = pl.BlockSpec(memory_space=pltpu.VMEM)
        dma = pltpu.SemaphoreType.DMA
        y_count = 9 * (n_y - 1)
        return pl.pallas_call(
            functools.partial(kernel, n_x, n_y),
            out_shape=pltpu.VMEM((rows, feats), BF16),
            in_specs=[any_spec, vmem_spec, any_spec, any_spec, any_spec,
                      vmem_spec, any_spec, any_spec, any_spec],
            out_specs=vmem_spec,
            scratch_shapes=[
                pltpu.VMEM((3, feats, ff), BF16),
                pltpu.VMEM((3, feats, ff), BF16),
                pltpu.VMEM((3, ff, feats), BF16),
                pltpu.VMEM((rows, feats), BF16),
                pltpu.VMEM((n_x, rows, feats), BF16),
                pltpu.VMEM((n_x, rows, feats), BF16),
                pltpu.VMEM((n_x - 1, rows, feats), BF16),
                pltpu.VMEM((rows, feats), BF16),
                pltpu.VMEM((wide, rows, feats), BF16),
                pltpu.VMEM((wide, rows, feats), BF16),
                pltpu.VMEM((wide - 1, rows, feats), BF16),
                pltpu.VMEM((shard, ff), BF16),
                pltpu.VMEM((shard, ff), BF16),
                pltpu.VMEM((ff, shard), BF16),
                pltpu.VMEM((2, rows, ff), BF16),
                pltpu.VMEM((2, 1, feats), F32),
                dma((7,)),
                dma(((n_x - 1) * SUBS,)),
                dma(((n_x - 1) * SUBS,)),
                dma(((wide - 1) * SUBS,)),
                dma(((wide - 1) * SUBS,)),
                dma((y_count,)),
                dma((9,)),
                dma((3,)),
                dma((3,)),
                dma,
                dma,
                dma,
                dma,
                dma((3,)),
                dma((3,)),
                dma((3,)),
                dma((3,)),
                pltpu.SemaphoreType.REGULAR,
            ],
            compiler_params=pltpu.CompilerParams(
                collective_id=0, has_side_effects=True, vmem_limit_bytes=60 * 1024 * 1024
            ),
        )(stream, gain1.reshape(-1, LANES), g1, u1, d1, gain2.reshape(-1, LANES), g2, u2, d2)

    tokens = P(("grp", "fs", "tp"), None)
    rows_split, cols_split = P("fs", "tp"), P("tp", "fs")
    in_specs = (
        tokens,
        P(), rows_split, rows_split, cols_split,
        P(), rows_split, rows_split, cols_split,
    )
    return jax.shard_map(local, mesh=mesh, in_specs=in_specs, out_specs=tokens, check_vma=False)
```

```python
import functools

import jax
import jax.numpy as jnp
from jax import lax
from jax.experimental import pallas as pl
from jax.experimental.pallas import tpu as pltpu
from jax.sharding import PartitionSpec as P

MESH = pl.DeviceIdType.MESH
F32 = jnp.float32
BF16 = jnp.bfloat16
SUBS = 4
CORES = 2
LANES = 128


def rms_norm(rows_f, gain):
    scale = lax.rsqrt(jnp.mean(rows_f * rows_f, axis=-1, keepdims=True) + 1e-06)
    return (rows_f * scale * gain).astype(BF16)


def kernel(
    n_x, n_y,
    stream, gain1, g1, u1, d1, gain2, g2, u2, d2,
    out,
    wg, wu, wd, st, x1, p1, s1, mid, x2, p2, s2, rg, ru, rd, hid, gains,
    load_sem, tok_recv, y_recv, sib_recv, rel_recv, fin_recv,
    ag1_send, rs1_send, ag2_send, rs2_send, y_send, sib_send, rel_send, fin_send, both_in, leap_in,
):
    x = lax.axis_index("tp")
    f = lax.axis_index("fs")
    y = f // CORES
    c = f % CORES
    d = 1 - 2 * c
    hops = n_x - 1
    wide = n_x // 2
    leap = n_x // 4
    rows = st.shape[0]
    sub = rows // SUBS
    shard = g1.shape[0]
    y_hops = n_y - 1

    x_near = ({"tp": (x + 1) % n_x}, {"tp": (x - 1 + n_x) % n_x})
    x_leap = {"tp": (x + leap * d + n_x) % n_x}
    y_next = {"fs": CORES * ((y + d + n_y) % n_y) + c}
    y_prev = {"fs": CORES * ((y - d + n_y) % n_y) + c}
    sibling = {"fs": CORES * y + 1 - c}

    def remote(src, dst, send, recv, device):
        return pltpu.make_async_remote_copy(
            src_ref=src, dst_ref=dst, send_sem=send, recv_sem=recv,
            device_id=device, device_id_type=MESH,
        )

    def piece(w, mat, owner):
        span = pl.ds(pl.multiple_of(owner * shard, shard), shard)
        if mat == 0:
            return wg.at[w, span, :]
        if mat == 1:
            return wu.at[w, span, :]
        return wd.at[w, :, span]

    def many(w, mat, count):
        span = pl.ds(0, count * shard)
        if mat == 0:
            return wg.at[w, span, :]
        if mat == 1:
            return wu.at[w, span, :]
        return wd.at[w, :, span]

    bit = sub // 2

    class Halves:
        def __init__(self, src, src_k, dst, dst_k, m, send, recv, slot, back=False):
            self.args = src, src_k, dst, dst_k, m, send, recv, slot, back

        def start(self):
            src, src_k, dst, dst_k, m, send, recv, slot, back = self.args
            for way in range(2):
                span = pl.ds(pl.multiple_of(m * sub, sub) + way * bit, bit)
                remote(
                    src.at[src_k, span, :], dst.at[dst_k, span, :], send,
                    recv.at[slot], x_near[1 - way if back else way],
                ).start()

        def wait_recv(self):
            _, _, dst, dst_k, m, send, recv, slot, _ = self.args
            whole = dst.at[dst_k, pl.ds(pl.multiple_of(m * sub, sub), sub), :]
            remote(whole, whole, send, recv.at[slot], x_near[0]).wait_recv()

    def relay_on(came, goes):
        came.wait_recv()
        goes.start()

    barrier = pltpu.get_barrier_semaphore()
    partners = [x_near[0], x_near[1], y_next, y_prev]
    assert leap <= 2
    for device in partners:
        pl.semaphore_signal(barrier, inc=1, device_id=device, device_id_type=MESH)

    @pl.when(c == 1)
    def _():
        witness = {"fs": CORES * y, "tp": (x + 1) % n_x}
        pl.semaphore_signal(barrier, inc=1, device_id=witness, device_id_type=MESH)

    loads = [pltpu.make_async_copy(stream, st, load_sem.at[0])]
    for i, (src, w, mat) in enumerate(
        ((g1, 0, 0), (u1, 0, 1), (d1, 0, 2), (g2, 1, 0), (u2, 1, 1), (d2, 1, 2))
    ):
        loads.append(pltpu.make_async_copy(src, piece(w, mat, f), load_sem.at[1 + i]))
    for copy in loads:
        copy.start()
    for i, gain in enumerate((gain1, gain2)):
        for j in range(gain.shape[0]):
            gains[i, :, j * LANES:(j + 1) * LANES] = gain[j:j + 1, :].astype(F32)
    pl.semaphore_wait(barrier, len(partners) + 1 - c)
    pl.semaphore_signal(leap_in, inc=1, device_id={"tp": (x - d + n_x) % n_x}, device_id_type=MESH)

    @pl.when(c == 0)
    def _():
        for core in range(CORES):
            device = {"fs": CORES * y + core, "tp": (x - 1 + n_x) % n_x}
            pl.semaphore_signal(both_in, inc=1, device_id=device, device_id_type=MESH)

    head = 4
    first_ticks = head * y_hops
    all_ticks = 9 * y_hops

    def share(w, mat, owner):
        ref = piece(w, mat, owner)
        remote(ref, ref, sib_send.at[mat], sib_recv.at[w * 3 + mat], sibling).start()

    def pass_on(w, mat, owner, n):
        ref = piece(w, mat, owner)
        remote(ref, ref, y_send.at[mat], y_recv.at[n], y_next).start()

    def share_item(i):
        owner = CORES * ((y - d * (i // head) + CORES * n_y) % n_y) + c
        item = i % head
        for mat in range(3):
            @pl.when(item % 3 == mat)
            def _():
                share(item // 3, mat, owner)

    def own(item):
        w, mat = item // 3, item % 3
        if w == 2:
            ref = piece(2, mat, f)
            remote(ref, ref, fin_send.at[mat], fin_recv.at[mat], x_leap).wait_recv()
        if item < head:
            pass_on(w, mat, f, item)
        else:
            pass_on(w, mat, f, first_ticks + item - head)
            share(w, mat, f)

    def y_tick(n, sharing=True):
        late = n >= first_ticks
        r = n - jnp.where(late, first_ticks, 0)
        step = jnp.where(late, r // (9 - head), r // head)
        size = jnp.where(late, 9 - head, head)
        item = r - step * size + jnp.where(late, head, 0)
        w = item // 3
        owner = CORES * ((y - d * (step + 1) + CORES * n_y) % n_y) + c

        def arrived(mat):
            ref = piece(w, mat, owner)
            remote(ref, ref, y_send.at[mat], y_recv.at[n], y_next).wait_recv()

            @pl.when(step < y_hops - 1)
            def _():
                pass_on(w, mat, owner, n + size)

            if sharing is True:
                share(w, mat, owner)
            else:
                @pl.when(sharing)
                def _():
                    share(w, mat, owner)

        for mat in range(3):
            @pl.when((n < all_ticks) & (item % 3 == mat))
            def _():
                arrived(mat)

        for item_own in range(head, 9):
            @pl.when((n < first_ticks) & (step == y_hops - 1) & (item == min(item_own - head, head - 1)))
            def _():
                own(item_own)

    def wait_siblings(w):
        for mat in range(3):
            ref = many(w, mat, n_y)
            remote(ref, ref, sib_send.at[mat], sib_recv.at[w * 3 + mat], sibling).wait_recv()

    def ag1_copy(k, m):
        return Halves(x1, k, x1, k + 1, m, ag1_send, tok_recv, k * SUBS + m)

    loads[0].wait()
    for m in range(SUBS):
        part = pl.ds(m * sub, sub)
        x1[0, part, :] = rms_norm(st[part, :].astype(F32), gains[0])
        ag1_copy(0, m).start()
        if m == 0:
            for item in range(head):
                loads[1 + item].wait()
                own(item)

    relay = (rg, ru, rd)
    pl.semaphore_wait(leap_in, 1)
    for mat in range(3):
        if mat:
            loads[4 + mat].wait()
        remote(piece(1, mat, f), relay[mat], rel_send.at[mat], rel_recv.at[mat], x_leap).start()

    def ag1_tick(k, m, last):
        if last:
            ag1_copy(k - 1, m).wait_recv()
        else:
            relay_on(ag1_copy(k - 1, m), ag1_copy(k, m))

    relay_at = max(1, n_y // 2 - 1)
    share_at = max(1, min(relay_at + 1, hops - 2))

    pause = 3 * leap

    def extra(n, count, sharing):
        def body(i, carry):
            y_tick(n + i, sharing)
            return carry
        lax.fori_loop(0, count, body, 0)

    def gather_first(k, n):
        @pl.when(k == relay_at)
        def _():
            for mat in range(3):
                remote(relay[mat], relay[mat], rel_send.at[mat], rel_recv.at[mat], x_leap).wait_recv()
                remote(relay[mat], piece(2, mat, f), fin_send.at[mat], fin_recv.at[mat], x_leap).start()

        @pl.when(k == share_at)
        def _():
            pl.semaphore_wait(both_in, 1)

            def body(i, carry):
                share_item(i)
                return carry
            lax.fori_loop(0, jnp.maximum(n, 0) + head, body, 0)

        late = (k == 2) | (k == relay_at + 1)

        @pl.when(late)
        def _():
            extra(n, pause, k >= share_at)

        n = n + jnp.where(late, pause, 0)
        for m in range(SUBS):
            ag1_tick(k, m, False)

            @pl.when((k > 1) | (m >= SUBS // 2))
            def _():
                y_tick(n + m, k >= share_at)
        return n + SUBS

    def rest(n, carry):
        y_tick(n)
        return carry

    ticks = lax.fori_loop(1, hops - 1, gather_first, -(SUBS // 2))
    lax.fori_loop(ticks, first_ticks, rest, 0)
    ticks = jnp.maximum(ticks, first_ticks)
    wait_siblings(0)

    def hidden_part(tokens, w, lo, width):
        gate = jnp.dot(tokens, wg[w, :, lo:lo + width], preferred_element_type=F32)
        up = jnp.dot(tokens, wu[w, :, lo:lo + width], preferred_element_type=F32)
        return ((gate / (1.0 + jnp.exp(-gate))) * up).astype(BF16)

    ff = wg.shape[2]
    feats = wd.shape[2]

    def first_quarter(k, m):
        if m < 2:
            width = ff // 2
            lo = m * width
            hid[0, :, lo:lo + width] = hidden_part(x1[k], 0, lo, width)
        else:
            width = feats // 2
            lo = (m - 2) * width
            p1[k, :, lo:lo + width] = jnp.dot(
                hid[0], wd[0, :, lo:lo + width], preferred_element_type=F32
            ).astype(BF16)

    def rs1_copy(src, src_k, k, m):
        return Halves(src, src_k, s1, k - 1, m, rs1_send, tok_recv, (k - 1) * SUBS + m)

    def reduce_first(j, n):
        for m in range(SUBS):
            @pl.when(j == 0)
            def _():
                ag1_tick(hops - 1, m, False)

            @pl.when(j == 1)
            def _():
                ag1_tick(hops, m, True)
                rs1_copy(p1, 1, 1, m).start()

            @pl.when(j >= 2)
            def _():
                part = pl.ds(m * sub, sub)
                rs1_copy(s1, j - 2, j - 1, m).wait_recv()
                s1[j - 2, part, :] = (
                    s1[j - 2, part, :].astype(F32) + p1[j, part, :].astype(F32)
                ).astype(BF16)
                rs1_copy(s1, j - 2, j, m).start()

            y_tick(n + m)
            first_quarter((j + 1) % n_x, m)
        return n + SUBS

    ticks = lax.fori_loop(0, n_x, reduce_first, ticks)

    def ag2_copy(t):
        k, m = t // SUBS, t % SUBS
        return Halves(x2, k, x2, k + 1, m, ag2_send, tok_recv, t)

    for m in range(SUBS):
        part = pl.ds(m * sub, sub)
        rs1_copy(s1, hops - 1, hops, m).wait_recv()
        total = s1[hops - 1, part, :].astype(F32) + p1[0, part, :].astype(F32)
        middle = (st[part, :].astype(F32) + 0.5 * total).astype(BF16)
        mid[part, :] = middle
        x2[0, part, :] = rms_norm(middle.astype(F32), gains[1])
        ag2_copy(m).start()
        y_tick(ticks + m)

    passes = (wide - 2) * SUBS

    def ag2_tick(t):
        @pl.when(t < passes)
        def _():
            relay_on(ag2_copy(t), ag2_copy(t + SUBS))

    for t in range(SUBS):
        ag2_tick(t)

    lax.fori_loop(ticks + SUBS, all_ticks, rest, 0)
    wait_siblings(1)
    wait_siblings(2)

    def second_quarter(k, m, lo_row, count):
        tokens = pl.ds(lo_row, count)
        if m < 2:
            width = ff // 2 if count == rows else ff
            for lo in range(0, ff, width):
                hid[m, tokens, lo:lo + width] = hidden_part(x2[k, tokens, :], 1 + m, lo, width)
        else:
            width = feats // 2
            lo = (m - 2) * width
            p2[k, tokens, lo:lo + width] = (
                jnp.dot(hid[0, tokens, :], wd[1, :, lo:lo + width], preferred_element_type=F32)
                + jnp.dot(hid[1, tokens, :], wd[2, :, lo:lo + width], preferred_element_type=F32)
            ).astype(BF16)

    for t in range(SUBS, passes):
        ag2_tick(t)
    for q in range(4 if wide > 2 else 0):
        second_quarter(wide - 2, q, 0, rows)

    def rs2_copy(src, k, m):
        return Halves(src, k, s2, k - 1, m, rs2_send, tok_recv, (wide + k - 2) * SUBS + m, back=True)

    half = rows // 2

    def last_block(h, carry):
        for m in range(SUBS // 2):
            ag2_copy(passes + h * (SUBS // 2) + m).wait_recv()
        for q in range(4):
            second_quarter(wide - 1, q, pl.multiple_of(h * half, half), half)
        for m in range(SUBS // 2):
            rs2_copy(p2, wide - 1, h * (SUBS // 2) + m).start()
        return carry

    lax.fori_loop(0, 2, last_block, 0)

    def sent(ref, sem):
        remote(ref, ref, sem, rel_recv.at[0], sibling).wait_send()

    sent(x1.at[pl.ds(0, hops)], ag1_send)
    sent(s1, rs1_send)
    sent(x2.at[pl.ds(0, wide - 1)], ag2_send)
    for mat in range(3):
        sent(relay[mat], rel_send.at[mat])
        sent(relay[mat], fin_send.at[mat])
        sent(many(pl.ds(0, 3), mat, y_hops), y_send.at[mat])
        sent(many(pl.ds(0, 3), mat, n_y), sib_send.at[mat])

    def reduce_second(i, carry):
        k = wide - 2 - i
        for m in range(SUBS):
            part = pl.ds(m * sub, sub)
            rs2_copy(s2, k + 1, m).wait_recv()
            s2[k, part, :] = (
                s2[k, part, :].astype(F32) + p2[k, part, :].astype(F32)
            ).astype(BF16)
            rs2_copy(s2, k, m).start()
            second_quarter(k - 1, m, 0, rows)
        return carry

    if wide > 2:
        lax.fori_loop(0, wide - 2, reduce_second, 0)
    else:
        for q in range(4):
            second_quarter(0, q, 0, rows)

    for m in range(SUBS):
        part = pl.ds(m * sub, sub)
        rs2_copy(s2, 1, m).wait_recv()
        total = s2[0, part, :].astype(F32) + p2[0, part, :].astype(F32)
        out[part, :] = (mid[part, :].astype(F32) + 0.5 * total).astype(BF16)

    sent(s2, rs2_send)


def solution(mesh):
    n_x = mesh.shape["tp"]
    n_y = mesh.shape["fs"] // CORES

    def local(stream, gain1, g1, u1, d1, gain2, g2, u2, d2):
        rows, feats = stream.shape
        shard, ff = g1.shape
        wide = n_x // 2
        any_spec = pl.BlockSpec(memory_space=pl.ANY)
        vmem_spec = pl.BlockSpec(memory_space=pltpu.VMEM)
        dma = pltpu.SemaphoreType.DMA
        y_count = 9 * (n_y - 1)
        return pl.pallas_call(
            functools.partial(kernel, n_x, n_y),
            out_shape=pltpu.VMEM((rows, feats), BF16),
            in_specs=[any_spec, vmem_spec, any_spec, any_spec, any_spec,
                      vmem_spec, any_spec, any_spec, any_spec],
            out_specs=vmem_spec,
            scratch_shapes=[
                pltpu.VMEM((3, feats, ff), BF16),
                pltpu.VMEM((3, feats, ff), BF16),
                pltpu.VMEM((3, ff, feats), BF16),
                pltpu.VMEM((rows, feats), BF16),
                pltpu.VMEM((n_x, rows, feats), BF16),
                pltpu.VMEM((n_x, rows, feats), BF16),
                pltpu.VMEM((n_x - 1, rows, feats), BF16),
                pltpu.VMEM((rows, feats), BF16),
                pltpu.VMEM((wide, rows, feats), BF16),
                pltpu.VMEM((wide, rows, feats), BF16),
                pltpu.VMEM((wide - 1, rows, feats), BF16),
                pltpu.VMEM((shard, ff), BF16),
                pltpu.VMEM((shard, ff), BF16),
                pltpu.VMEM((ff, shard), BF16),
                pltpu.VMEM((2, rows, ff), BF16),
                pltpu.VMEM((2, 1, feats), F32),
                dma((7,)),
                dma(((n_x - 1) * SUBS,)),
                dma((y_count,)),
                dma((9,)),
                dma((3,)),
                dma((3,)),
                dma,
                dma,
                dma,
                dma,
                dma((3,)),
                dma((3,)),
                dma((3,)),
                dma((3,)),
                pltpu.SemaphoreType.REGULAR,
                pltpu.SemaphoreType.REGULAR,
            ],
            compiler_params=pltpu.CompilerParams(
                collective_id=0, has_side_effects=True, vmem_limit_bytes=60 * 1024 * 1024
            ),
        )(stream, gain1.reshape(-1, LANES), g1, u1, d1, gain2.reshape(-1, LANES), g2, u2, d2)

    tokens = P(("grp", "fs", "tp"), None)
    rows_split, cols_split = P("fs", "tp"), P("tp", "fs")
    in_specs = (
        tokens,
        P(), rows_split, rows_split, cols_split,
        P(), rows_split, rows_split, cols_split,
    )
    return jax.shard_map(local, mesh=mesh, in_specs=in_specs, out_specs=tokens, check_vma=False)
```

```python
import functools

import jax
import jax.numpy as jnp
from jax import lax
from jax.experimental import pallas as pl
from jax.experimental.pallas import tpu as pltpu
from jax.sharding import PartitionSpec as P

MESH = pl.DeviceIdType.MESH
F32 = jnp.float32
BF16 = jnp.bfloat16
SUBS = 4
CORES = 2
LANES = 128


def rms_norm(rows_f, gain):
    scale = lax.rsqrt(jnp.mean(rows_f * rows_f, axis=-1, keepdims=True) + 1e-06)
    return (rows_f * scale * gain).astype(BF16)


def kernel(
    n_x, n_y,
    stream, gain1, g1, u1, d1, gain2, g2, u2, d2,
    out,
    wg, wu, wd, st, x1, p1, s1, mid, x2, p2, s2, rg, ru, rd, hid, raw, gains,
    load_sem, tok_recv, y_recv, sib_recv, rel_recv, fin_recv,
    ag1_send, rs1_send, ag2_send, rs2_send, y_send, sib_send, rel_send, fin_send, both_in, leap_in,
):
    x = lax.axis_index("tp")
    f = lax.axis_index("fs")
    y = f // CORES
    c = f % CORES
    d = 1 - 2 * c
    hops = n_x - 1
    wide = n_x // 2
    leap = n_x // 4
    rows = st.shape[0]
    sub = rows // SUBS
    shard = g1.shape[0]
    y_hops = n_y - 1

    x_near = ({"tp": (x + 1) % n_x}, {"tp": (x - 1 + n_x) % n_x})
    x_leap = {"tp": (x + leap * d + n_x) % n_x}
    y_next = {"fs": CORES * ((y + d + n_y) % n_y) + c}
    y_prev = {"fs": CORES * ((y - d + n_y) % n_y) + c}
    sibling = {"fs": CORES * y + 1 - c}

    def remote(src, dst, send, recv, device):
        return pltpu.make_async_remote_copy(
            src_ref=src, dst_ref=dst, send_sem=send, recv_sem=recv,
            device_id=device, device_id_type=MESH,
        )

    def piece(w, mat, owner):
        span = pl.ds(pl.multiple_of(owner * shard, shard), shard)
        if mat == 0:
            return wg.at[w, span, :]
        if mat == 1:
            return wu.at[w, span, :]
        return wd.at[w, :, span]

    def many(w, mat, count):
        span = pl.ds(0, count * shard)
        if mat == 0:
            return wg.at[w, span, :]
        if mat == 1:
            return wu.at[w, span, :]
        return wd.at[w, :, span]

    bit = sub // 2

    class Halves:
        def __init__(self, src, src_k, dst, dst_k, m, send, recv, slot, back=False):
            self.args = src, src_k, dst, dst_k, m, send, recv, slot, back

        def start(self):
            src, src_k, dst, dst_k, m, send, recv, slot, back = self.args
            for way in range(2):
                span = pl.ds(pl.multiple_of(m * sub, sub) + way * bit, bit)
                remote(
                    src.at[src_k, span, :], dst.at[dst_k, span, :], send,
                    recv.at[slot], x_near[1 - way if back else way],
                ).start()

        def wait_recv(self):
            _, _, dst, dst_k, m, send, recv, slot, _ = self.args
            whole = dst.at[dst_k, pl.ds(pl.multiple_of(m * sub, sub), sub), :]
            remote(whole, whole, send, recv.at[slot], x_near[0]).wait_recv()

    def relay_on(came, goes):
        came.wait_recv()
        goes.start()

    barrier = pltpu.get_barrier_semaphore()
    partners = [x_near[0], x_near[1], y_next, y_prev]
    assert leap <= 2
    for device in partners:
        pl.semaphore_signal(barrier, inc=1, device_id=device, device_id_type=MESH)

    @pl.when(c == 1)
    def _():
        witness = {"fs": CORES * y, "tp": (x + 1) % n_x}
        pl.semaphore_signal(barrier, inc=1, device_id=witness, device_id_type=MESH)

    loads = [pltpu.make_async_copy(stream, st, load_sem.at[0])]
    for i, (src, w, mat) in enumerate(
        ((g1, 0, 0), (u1, 0, 1), (d1, 0, 2), (g2, 1, 0), (u2, 1, 1), (d2, 1, 2))
    ):
        loads.append(pltpu.make_async_copy(src, piece(w, mat, f), load_sem.at[1 + i]))
    for i, gain in enumerate((gain1, gain2)):
        loads.append(pltpu.make_async_copy(gain, raw.at[i], load_sem.at[7 + i]))
    for copy in loads:
        copy.start()

    loads[7].wait()
    loads[8].wait()
    for i in range(2):
        for j in range(raw.shape[1]):
            gains[i, :, j * LANES:(j + 1) * LANES] = raw[i, j:j + 1, :].astype(F32)
    loads[0].wait()
    for m in range(SUBS):
        part = pl.ds(m * sub, sub)
        x1[0, part, :] = rms_norm(st[part, :].astype(F32), gains[0])
    pl.semaphore_wait(barrier, len(partners) + 1 - c)
    pl.semaphore_signal(leap_in, inc=1, device_id={"tp": (x - d + n_x) % n_x}, device_id_type=MESH)

    @pl.when(c == 0)
    def _():
        for core in range(CORES):
            device = {"fs": CORES * y + core, "tp": (x - 1 + n_x) % n_x}
            pl.semaphore_signal(both_in, inc=1, device_id=device, device_id_type=MESH)

    head = 4
    first_ticks = head * y_hops
    all_ticks = 9 * y_hops

    def share(w, mat, owner):
        ref = piece(w, mat, owner)
        remote(ref, ref, sib_send.at[mat], sib_recv.at[w * 3 + mat], sibling).start()

    def pass_on(w, mat, owner, n):
        ref = piece(w, mat, owner)
        remote(ref, ref, y_send.at[mat], y_recv.at[n], y_next).start()

    def share_item(i):
        owner = CORES * ((y - d * (i // head) + CORES * n_y) % n_y) + c
        item = i % head
        for mat in range(3):
            @pl.when(item % 3 == mat)
            def _():
                share(item // 3, mat, owner)

    def own(item):
        w, mat = item // 3, item % 3
        if w == 2:
            ref = piece(2, mat, f)
            remote(ref, ref, fin_send.at[mat], fin_recv.at[mat], x_leap).wait_recv()
        if item < head:
            pass_on(w, mat, f, item)
        else:
            pass_on(w, mat, f, first_ticks + item - head)
            share(w, mat, f)

    def y_tick(n, sharing=True):
        late = n >= first_ticks
        r = n - jnp.where(late, first_ticks, 0)
        step = jnp.where(late, r // (9 - head), r // head)
        size = jnp.where(late, 9 - head, head)
        item = r - step * size + jnp.where(late, head, 0)
        w = item // 3
        owner = CORES * ((y - d * (step + 1) + CORES * n_y) % n_y) + c

        def arrived(mat):
            ref = piece(w, mat, owner)
            remote(ref, ref, y_send.at[mat], y_recv.at[n], y_next).wait_recv()

            @pl.when(step < y_hops - 1)
            def _():
                pass_on(w, mat, owner, n + size)

            if sharing is True:
                share(w, mat, owner)
            else:
                @pl.when(sharing)
                def _():
                    share(w, mat, owner)

        for mat in range(3):
            @pl.when((n < all_ticks) & (item % 3 == mat))
            def _():
                arrived(mat)

        for item_own in range(head, 9):
            @pl.when((n < first_ticks) & (step == y_hops - 1) & (item == min(item_own - head, head - 1)))
            def _():
                own(item_own)

    def wait_siblings(w):
        for mat in range(3):
            ref = many(w, mat, n_y)
            remote(ref, ref, sib_send.at[mat], sib_recv.at[w * 3 + mat], sibling).wait_recv()

    def ag1_copy(k, m):
        return Halves(x1, k, x1, k + 1, m, ag1_send, tok_recv, k * SUBS + m)

    for m in range(SUBS):
        ag1_copy(0, m).start()
        if m == 0:
            for item in range(head):
                loads[1 + item].wait()
                own(item)

    relay = (rg, ru, rd)
    pl.semaphore_wait(leap_in, 1)
    for mat in range(3):
        if mat:
            loads[4 + mat].wait()
        remote(piece(1, mat, f), relay[mat], rel_send.at[mat], rel_recv.at[mat], x_leap).start()

    def ag1_tick(k, m, last):
        if last:
            ag1_copy(k - 1, m).wait_recv()
        else:
            relay_on(ag1_copy(k - 1, m), ag1_copy(k, m))

    relay_at = max(1, n_y // 2 - 1)
    share_at = max(1, min(relay_at + 1, hops - 2))

    pause = 3 * leap

    def extra(n, count, sharing):
        def body(i, carry):
            y_tick(n + i, sharing)
            return carry
        lax.fori_loop(0, count, body, 0)

    def gather_first(k, n):
        @pl.when(k == relay_at)
        def _():
            for mat in range(3):
                remote(relay[mat], relay[mat], rel_send.at[mat], rel_recv.at[mat], x_leap).wait_recv()
                remote(relay[mat], piece(2, mat, f), fin_send.at[mat], fin_recv.at[mat], x_leap).start()

        @pl.when(k == share_at)
        def _():
            pl.semaphore_wait(both_in, 1)

            def body(i, carry):
                share_item(i)
                return carry
            lax.fori_loop(0, jnp.maximum(n, 0) + head, body, 0)

        late = (k == 2) | (k == relay_at + 1)

        @pl.when(late)
        def _():
            extra(n, pause, k >= share_at)

        n = n + jnp.where(late, pause, 0)
        for m in range(SUBS):
            ag1_tick(k, m, False)

            @pl.when((k > 1) | (m >= SUBS // 2))
            def _():
                y_tick(n + m, k >= share_at)
        return n + SUBS

    def rest(n, carry):
        y_tick(n)
        return carry

    ticks = lax.fori_loop(1, hops - 1, gather_first, -(SUBS // 2))
    lax.fori_loop(ticks, first_ticks, rest, 0)
    ticks = jnp.maximum(ticks, first_ticks)
    wait_siblings(0)

    def hidden_part(tokens, w, lo, width):
        gate = jnp.dot(tokens, wg[w, :, lo:lo + width], preferred_element_type=F32)
        up = jnp.dot(tokens, wu[w, :, lo:lo + width], preferred_element_type=F32)
        return ((gate / (1.0 + jnp.exp(-gate))) * up).astype(BF16)

    ff = wg.shape[2]
    feats = wd.shape[2]

    def first_quarter(k, m):
        if m < 2:
            width = ff // 2
            lo = m * width
            hid[0, :, lo:lo + width] = hidden_part(x1[k], 0, lo, width)
        else:
            width = feats // 2
            lo = (m - 2) * width
            p1[k, :, lo:lo + width] = jnp.dot(
                hid[0], wd[0, :, lo:lo + width], preferred_element_type=F32
            ).astype(BF16)

    def rs1_copy(src, src_k, k, m):
        return Halves(src, src_k, s1, k - 1, m, rs1_send, tok_recv, (k - 1) * SUBS + m)

    def reduce_first(j, n):
        for m in range(SUBS):
            @pl.when(j == 0)
            def _():
                ag1_tick(hops - 1, m, False)

            @pl.when(j == 1)
            def _():
                ag1_tick(hops, m, True)
                rs1_copy(p1, 1, 1, m).start()

            @pl.when(j >= 2)
            def _():
                part = pl.ds(m * sub, sub)
                rs1_copy(s1, j - 2, j - 1, m).wait_recv()
                s1[j - 2, part, :] = (
                    s1[j - 2, part, :].astype(F32) + p1[j, part, :].astype(F32)
                ).astype(BF16)
                rs1_copy(s1, j - 2, j, m).start()

            y_tick(n + m)
            first_quarter((j + 1) % n_x, m)
        return n + SUBS

    ticks = lax.fori_loop(0, n_x, reduce_first, ticks)

    def ag2_copy(t):
        k, m = t // SUBS, t % SUBS
        return Halves(x2, k, x2, k + 1, m, ag2_send, tok_recv, t)

    for m in range(SUBS):
        part = pl.ds(m * sub, sub)
        rs1_copy(s1, hops - 1, hops, m).wait_recv()
        total = s1[hops - 1, part, :].astype(F32) + p1[0, part, :].astype(F32)
        middle = (st[part, :].astype(F32) + 0.5 * total).astype(BF16)
        mid[part, :] = middle
        x2[0, part, :] = rms_norm(middle.astype(F32), gains[1])
        ag2_copy(m).start()
        y_tick(ticks + m)

    passes = (wide - 2) * SUBS

    def ag2_tick(t):
        @pl.when(t < passes)
        def _():
            relay_on(ag2_copy(t), ag2_copy(t + SUBS))

    for t in range(SUBS):
        ag2_tick(t)

    lax.fori_loop(ticks + SUBS, all_ticks, rest, 0)
    wait_siblings(1)
    wait_siblings(2)

    def second_quarter(k, m, lo_row, count):
        tokens = pl.ds(lo_row, count)
        if m < 2:
            width = ff // 2 if count == rows else ff
            for lo in range(0, ff, width):
                hid[m, tokens, lo:lo + width] = hidden_part(x2[k, tokens, :], 1 + m, lo, width)
        else:
            width = feats // 2
            lo = (m - 2) * width
            p2[k, tokens, lo:lo + width] = (
                jnp.dot(hid[0, tokens, :], wd[1, :, lo:lo + width], preferred_element_type=F32)
                + jnp.dot(hid[1, tokens, :], wd[2, :, lo:lo + width], preferred_element_type=F32)
            ).astype(BF16)

    for t in range(SUBS, passes):
        ag2_tick(t)
    for q in range(4 if wide > 2 else 0):
        second_quarter(wide - 2, q, 0, rows)

    def rs2_copy(src, k, m):
        return Halves(src, k, s2, k - 1, m, rs2_send, tok_recv, (wide + k - 2) * SUBS + m, back=True)

    half = rows // 2

    def last_block(h, carry):
        for m in range(SUBS // 2):
            ag2_copy(passes + h * (SUBS // 2) + m).wait_recv()
        for q in range(4):
            second_quarter(wide - 1, q, pl.multiple_of(h * half, half), half)
        for m in range(SUBS // 2):
            rs2_copy(p2, wide - 1, h * (SUBS // 2) + m).start()
        return carry

    lax.fori_loop(0, 2, last_block, 0)

    def sent(ref, sem):
        remote(ref, ref, sem, rel_recv.at[0], sibling).wait_send()

    sent(x1.at[pl.ds(0, hops)], ag1_send)
    sent(s1, rs1_send)
    sent(x2.at[pl.ds(0, wide - 1)], ag2_send)
    for mat in range(3):
        sent(relay[mat], rel_send.at[mat])
        sent(relay[mat], fin_send.at[mat])
        sent(many(pl.ds(0, 3), mat, y_hops), y_send.at[mat])
        sent(many(pl.ds(0, 3), mat, n_y), sib_send.at[mat])

    def reduce_second(i, carry):
        k = wide - 2 - i
        for m in range(SUBS):
            part = pl.ds(m * sub, sub)
            rs2_copy(s2, k + 1, m).wait_recv()
            s2[k, part, :] = (
                s2[k, part, :].astype(F32) + p2[k, part, :].astype(F32)
            ).astype(BF16)
            rs2_copy(s2, k, m).start()
            second_quarter(k - 1, m, 0, rows)
        return carry

    if wide > 2:
        lax.fori_loop(0, wide - 2, reduce_second, 0)
    else:
        for q in range(4):
            second_quarter(0, q, 0, rows)

    for m in range(SUBS):
        part = pl.ds(m * sub, sub)
        rs2_copy(s2, 1, m).wait_recv()
        total = s2[0, part, :].astype(F32) + p2[0, part, :].astype(F32)
        out[part, :] = (mid[part, :].astype(F32) + 0.5 * total).astype(BF16)

    sent(s2, rs2_send)


def solution(mesh):
    n_x = mesh.shape["tp"]
    n_y = mesh.shape["fs"] // CORES

    def local(stream, gain1, g1, u1, d1, gain2, g2, u2, d2):
        rows, feats = stream.shape
        shard, ff = g1.shape
        wide = n_x // 2
        any_spec = pl.BlockSpec(memory_space=pl.ANY)
        vmem_spec = pl.BlockSpec(memory_space=pltpu.VMEM)
        dma = pltpu.SemaphoreType.DMA
        y_count = 9 * (n_y - 1)
        return pl.pallas_call(
            functools.partial(kernel, n_x, n_y),
            out_shape=pltpu.VMEM((rows, feats), BF16),
            in_specs=[any_spec] * 9,
            out_specs=vmem_spec,
            scratch_shapes=[
                pltpu.VMEM((3, feats, ff), BF16),
                pltpu.VMEM((3, feats, ff), BF16),
                pltpu.VMEM((3, ff, feats), BF16),
                pltpu.VMEM((rows, feats), BF16),
                pltpu.VMEM((n_x, rows, feats), BF16),
                pltpu.VMEM((n_x, rows, feats), BF16),
                pltpu.VMEM((n_x - 1, rows, feats), BF16),
                pltpu.VMEM((rows, feats), BF16),
                pltpu.VMEM((wide, rows, feats), BF16),
                pltpu.VMEM((wide, rows, feats), BF16),
                pltpu.VMEM((wide - 1, rows, feats), BF16),
                pltpu.VMEM((shard, ff), BF16),
                pltpu.VMEM((shard, ff), BF16),
                pltpu.VMEM((ff, shard), BF16),
                pltpu.VMEM((2, rows, ff), BF16),
                pltpu.VMEM((2, feats // LANES, LANES), BF16),
                pltpu.VMEM((2, 1, feats), F32),
                dma((9,)),
                dma(((n_x - 1) * SUBS,)),
                dma((y_count,)),
                dma((9,)),
                dma((3,)),
                dma((3,)),
                dma,
                dma,
                dma,
                dma,
                dma((3,)),
                dma((3,)),
                dma((3,)),
                dma((3,)),
                pltpu.SemaphoreType.REGULAR,
                pltpu.SemaphoreType.REGULAR,
            ],
            compiler_params=pltpu.CompilerParams(
                collective_id=0, has_side_effects=True, vmem_limit_bytes=60 * 1024 * 1024
            ),
        )(stream, gain1.reshape(-1, LANES), g1, u1, d1, gain2.reshape(-1, LANES), g2, u2, d2)

    tokens = P(("grp", "fs", "tp"), None)
    rows_split, cols_split = P("fs", "tp"), P("tp", "fs")
    in_specs = (
        tokens,
        P(), rows_split, rows_split, cols_split,
        P(), rows_split, rows_split, cols_split,
    )
    return jax.shard_map(local, mesh=mesh, in_specs=in_specs, out_specs=tokens, check_vma=False)
```

```python
import functools

import jax
import jax.numpy as jnp
from jax import lax
from jax.experimental import pallas as pl
from jax.experimental.pallas import tpu as pltpu
from jax.sharding import PartitionSpec as P

MESH = pl.DeviceIdType.MESH
F32 = jnp.float32
BF16 = jnp.bfloat16
SUBS = 4
CORES = 2
LANES = 128


def rms_norm(rows_f, gain):
    scale = lax.rsqrt(jnp.mean(rows_f * rows_f, axis=-1, keepdims=True) + 1e-06)
    return (rows_f * scale * gain).astype(BF16)


def kernel(
    n_x, n_y,
    stream, gain1, g1, u1, d1, gain2, g2, u2, d2,
    out,
    wg, wu, wd, st, x1, p1, s1, mid, x2, p2, s2, rg, ru, rd, hid, raw, gains,
    load_sem, tok_recv, y_recv, sib_recv, rel_recv, fin_recv,
    ag1_send, rs1_send, ag2_send, rs2_send, y_send, sib_send, rel_send, fin_send, both_in, leap_in,
):
    x = lax.axis_index("tp")
    f = lax.axis_index("fs")
    y = f // CORES
    c = f % CORES
    d = 1 - 2 * c
    hops = n_x - 1
    wide = n_x // 2
    leap = n_x // 4
    rows = st.shape[0]
    sub = rows // SUBS
    shard = g1.shape[0]
    y_hops = n_y - 1

    x_near = ({"tp": (x + 1) % n_x}, {"tp": (x - 1 + n_x) % n_x})
    x_leap = {"tp": (x + leap * d + n_x) % n_x}
    y_next = {"fs": CORES * ((y + d + n_y) % n_y) + c}
    y_prev = {"fs": CORES * ((y - d + n_y) % n_y) + c}
    sibling = {"fs": CORES * y + 1 - c}

    def remote(src, dst, send, recv, device):
        return pltpu.make_async_remote_copy(
            src_ref=src, dst_ref=dst, send_sem=send, recv_sem=recv,
            device_id=device, device_id_type=MESH,
        )

    def piece(w, mat, owner):
        span = pl.ds(pl.multiple_of(owner * shard, shard), shard)
        if mat == 0:
            return wg.at[w, span, :]
        if mat == 1:
            return wu.at[w, span, :]
        return wd.at[w, :, span]

    def many(w, mat, count):
        span = pl.ds(0, count * shard)
        if mat == 0:
            return wg.at[w, span, :]
        if mat == 1:
            return wu.at[w, span, :]
        return wd.at[w, :, span]

    bit = sub // 2

    class Halves:
        def __init__(self, src, src_k, dst, dst_k, m, send, recv, slot, back=False):
            self.args = src, src_k, dst, dst_k, m, send, recv, slot, back

        def start(self):
            src, src_k, dst, dst_k, m, send, recv, slot, back = self.args
            for way in range(2):
                span = pl.ds(pl.multiple_of(m * sub, sub) + way * bit, bit)
                remote(
                    src.at[src_k, span, :], dst.at[dst_k, span, :], send,
                    recv.at[slot], x_near[1 - way if back else way],
                ).start()

        def wait_recv(self):
            _, _, dst, dst_k, m, send, recv, slot, _ = self.args
            whole = dst.at[dst_k, pl.ds(pl.multiple_of(m * sub, sub), sub), :]
            remote(whole, whole, send, recv.at[slot], x_near[0]).wait_recv()

    def relay_on(came, goes):
        came.wait_recv()
        goes.start()

    barrier = pltpu.get_barrier_semaphore()
    partners = [x_near[0], x_near[1], y_next, y_prev]
    assert leap <= 2
    for device in partners:
        pl.semaphore_signal(barrier, inc=1, device_id=device, device_id_type=MESH)

    @pl.when(c == 1)
    def _():
        witness = {"fs": CORES * y, "tp": (x + 1) % n_x}
        pl.semaphore_signal(barrier, inc=1, device_id=witness, device_id_type=MESH)

    loads = [pltpu.make_async_copy(stream, st, load_sem.at[0])]
    for i, (src, w, mat) in enumerate(
        ((g1, 0, 0), (u1, 0, 1), (d1, 0, 2), (g2, 1, 0), (u2, 1, 1), (d2, 1, 2))
    ):
        loads.append(pltpu.make_async_copy(src, piece(w, mat, f), load_sem.at[1 + i]))
    for i, gain in enumerate((gain1, gain2)):
        loads.append(pltpu.make_async_copy(gain, raw.at[i], load_sem.at[7 + i]))
    for copy in loads:
        copy.start()

    loads[7].wait()
    loads[8].wait()
    for i in range(2):
        for j in range(raw.shape[1]):
            gains[i, :, j * LANES:(j + 1) * LANES] = raw[i, j:j + 1, :].astype(F32)
    loads[0].wait()
    for m in range(SUBS):
        part = pl.ds(m * sub, sub)
        x1[0, part, :] = rms_norm(st[part, :].astype(F32), gains[0])
    pl.semaphore_wait(barrier, len(partners) + 1 - c)
    pl.semaphore_signal(leap_in, inc=1, device_id={"tp": (x - d + n_x) % n_x}, device_id_type=MESH)

    @pl.when(c == 0)
    def _():
        for core in range(CORES):
            device = {"fs": CORES * y + core, "tp": (x - 1 + n_x) % n_x}
            pl.semaphore_signal(both_in, inc=1, device_id=device, device_id_type=MESH)

    head = 4
    first_ticks = head * y_hops
    all_ticks = 9 * y_hops

    def share(w, mat, owner):
        ref = piece(w, mat, owner)
        remote(ref, ref, sib_send.at[mat], sib_recv.at[w * 3 + mat], sibling).start()

    def pass_on(w, mat, owner, n):
        ref = piece(w, mat, owner)
        remote(ref, ref, y_send.at[mat], y_recv.at[n], y_next).start()

    def share_item(i):
        owner = CORES * ((y - d * (i // head) + CORES * n_y) % n_y) + c
        item = i % head
        for mat in range(3):
            @pl.when(item % 3 == mat)
            def _():
                share(item // 3, mat, owner)

    def own(item):
        w, mat = item // 3, item % 3
        if w == 2:
            ref = piece(2, mat, f)
            remote(ref, ref, fin_send.at[mat], fin_recv.at[mat], x_leap).wait_recv()
        if item < head:
            pass_on(w, mat, f, item)
        else:
            pass_on(w, mat, f, first_ticks + item - head)
            share(w, mat, f)

    def y_tick(n, sharing=True):
        late = n >= first_ticks
        r = n - jnp.where(late, first_ticks, 0)
        step = jnp.where(late, r // (9 - head), r // head)
        size = jnp.where(late, 9 - head, head)
        item = r - step * size + jnp.where(late, head, 0)
        w = item // 3
        owner = CORES * ((y - d * (step + 1) + CORES * n_y) % n_y) + c

        def arrived(mat):
            ref = piece(w, mat, owner)
            remote(ref, ref, y_send.at[mat], y_recv.at[n], y_next).wait_recv()

            @pl.when(step < y_hops - 1)
            def _():
                pass_on(w, mat, owner, n + size)

            if sharing is True:
                share(w, mat, owner)
            else:
                @pl.when(sharing)
                def _():
                    share(w, mat, owner)

        for mat in range(3):
            @pl.when((n < all_ticks) & (item % 3 == mat))
            def _():
                arrived(mat)

        for item_own in range(head, 9):
            @pl.when((n < first_ticks) & (step == y_hops - 1) & (item == min(item_own - head, head - 1)))
            def _():
                own(item_own)

    def wait_siblings(w):
        for mat in range(3):
            ref = many(w, mat, n_y)
            remote(ref, ref, sib_send.at[mat], sib_recv.at[w * 3 + mat], sibling).wait_recv()

    def ag1_copy(k, m):
        return Halves(x1, k, x1, k + 1, m, ag1_send, tok_recv, k % 2 * SUBS + m)

    for m in range(SUBS):
        ag1_copy(0, m).start()
        if m == 0:
            for item in range(head):
                loads[1 + item].wait()
                own(item)

    relay = (rg, ru, rd)
    pl.semaphore_wait(leap_in, 1)
    for mat in range(3):
        if mat:
            loads[4 + mat].wait()
        remote(piece(1, mat, f), relay[mat], rel_send.at[mat], rel_recv.at[mat], x_leap).start()

    def ag1_tick(k, m, last):
        if last:
            ag1_copy(k - 1, m).wait_recv()
        else:
            relay_on(ag1_copy(k - 1, m), ag1_copy(k, m))

    relay_at = max(1, n_y // 2 - 1)
    share_at = max(1, min(relay_at + 1, hops - 2))

    pause = 3 * leap

    def extra(n, count, sharing):
        def body(i, carry):
            y_tick(n + i, sharing)
            return carry
        lax.fori_loop(0, count, body, 0)

    def gather_first(k, n):
        @pl.when(k == relay_at)
        def _():
            for mat in range(3):
                remote(relay[mat], relay[mat], rel_send.at[mat], rel_recv.at[mat], x_leap).wait_recv()
                remote(relay[mat], piece(2, mat, f), fin_send.at[mat], fin_recv.at[mat], x_leap).start()

        @pl.when(k == share_at)
        def _():
            pl.semaphore_wait(both_in, 1)

            def body(i, carry):
                share_item(i)
                return carry
            lax.fori_loop(0, jnp.maximum(n, 0) + head, body, 0)

        late = (k == 2) | (k == relay_at + 1)

        @pl.when(late)
        def _():
            extra(n, pause, k >= share_at)

        n = n + jnp.where(late, pause, 0)
        for m in range(SUBS):
            ag1_tick(k, m, False)

            @pl.when((k > 1) | (m >= SUBS // 2))
            def _():
                y_tick(n + m, k >= share_at)
        return n + SUBS

    def rest(n, carry):
        y_tick(n)
        return carry

    ticks = lax.fori_loop(1, hops - 1, gather_first, -(SUBS // 2))
    lax.fori_loop(ticks, first_ticks, rest, 0)
    ticks = jnp.maximum(ticks, first_ticks)
    wait_siblings(0)

    def hidden_part(tokens, w, lo, width):
        gate = jnp.dot(tokens, wg[w, :, lo:lo + width], preferred_element_type=F32)
        up = jnp.dot(tokens, wu[w, :, lo:lo + width], preferred_element_type=F32)
        return ((gate / (1.0 + jnp.exp(-gate))) * up).astype(BF16)

    ff = wg.shape[2]
    feats = wd.shape[2]

    def first_quarter(k, m):
        if m < 2:
            width = ff // 2
            lo = m * width
            hid[0, :, lo:lo + width] = hidden_part(x1[k], 0, lo, width)
        else:
            width = feats // 2
            lo = (m - 2) * width
            p1[k, :, lo:lo + width] = jnp.dot(
                hid[0], wd[0, :, lo:lo + width], preferred_element_type=F32
            ).astype(BF16)

    def rs1_copy(src, src_k, k, m):
        return Halves(src, src_k, s1, k - 1, m, rs1_send, tok_recv, k % 2 * SUBS + m)

    def reduce_first(j, n):
        for m in range(SUBS):
            @pl.when(j == 0)
            def _():
                ag1_tick(hops - 1, m, False)

            @pl.when(j == 1)
            def _():
                ag1_tick(hops, m, True)
                rs1_copy(p1, 1, 1, m).start()

            @pl.when(j >= 2)
            def _():
                part = pl.ds(m * sub, sub)
                rs1_copy(s1, j - 2, j - 1, m).wait_recv()
                s1[j - 2, part, :] = (
                    s1[j - 2, part, :].astype(F32) + p1[j, part, :].astype(F32)
                ).astype(BF16)
                rs1_copy(s1, j - 2, j, m).start()

            y_tick(n + m)
            first_quarter((j + 1) % n_x, m)
        return n + SUBS

    ticks = lax.fori_loop(0, n_x, reduce_first, ticks)

    def ag2_copy(t):
        k, m = t // SUBS, t % SUBS
        return Halves(x2, k, x2, k + 1, m, ag2_send, tok_recv, k % 2 * SUBS + m)

    for m in range(SUBS):
        part = pl.ds(m * sub, sub)
        rs1_copy(s1, hops - 1, hops, m).wait_recv()
        total = s1[hops - 1, part, :].astype(F32) + p1[0, part, :].astype(F32)
        middle = (st[part, :].astype(F32) + 0.5 * total).astype(BF16)
        mid[part, :] = middle
        x2[0, part, :] = rms_norm(middle.astype(F32), gains[1])
        ag2_copy(m).start()
        y_tick(ticks + m)

    passes = (wide - 2) * SUBS

    def ag2_tick(t):
        @pl.when(t < passes)
        def _():
            relay_on(ag2_copy(t), ag2_copy(t + SUBS))

    for t in range(SUBS):
        ag2_tick(t)

    lax.fori_loop(ticks + SUBS, all_ticks, rest, 0)
    wait_siblings(1)
    wait_siblings(2)

    def second_quarter(k, m, lo_row, count):
        tokens = pl.ds(lo_row, count)
        if m < 2:
            width = ff // 2 if count == rows else ff
            for lo in range(0, ff, width):
                hid[m, tokens, lo:lo + width] = hidden_part(x2[k, tokens, :], 1 + m, lo, width)
        else:
            width = feats // 2
            lo = (m - 2) * width
            p2[k, tokens, lo:lo + width] = (
                jnp.dot(hid[0, tokens, :], wd[1, :, lo:lo + width], preferred_element_type=F32)
                + jnp.dot(hid[1, tokens, :], wd[2, :, lo:lo + width], preferred_element_type=F32)
            ).astype(BF16)

    for t in range(SUBS, passes):
        ag2_tick(t)
    for q in range(4 if wide > 2 else 0):
        second_quarter(wide - 2, q, 0, rows)

    def rs2_copy(src, k, m):
        return Halves(src, k, s2, k - 1, m, rs2_send, tok_recv, k % 2 * SUBS + m, back=True)

    half = rows // 2

    def last_block(h, carry):
        for m in range(SUBS // 2):
            ag2_copy(passes + h * (SUBS // 2) + m).wait_recv()
        for q in range(4):
            second_quarter(wide - 1, q, pl.multiple_of(h * half, half), half)
        for m in range(SUBS // 2):
            rs2_copy(p2, wide - 1, h * (SUBS // 2) + m).start()
        return carry

    lax.fori_loop(0, 2, last_block, 0)

    def sent(ref, sem):
        remote(ref, ref, sem, rel_recv.at[0], sibling).wait_send()

    sent(x1.at[pl.ds(0, hops)], ag1_send)
    sent(s1, rs1_send)
    sent(x2.at[pl.ds(0, wide - 1)], ag2_send)
    for mat in range(3):
        sent(relay[mat], rel_send.at[mat])
        sent(relay[mat], fin_send.at[mat])
        sent(many(pl.ds(0, 3), mat, y_hops), y_send.at[mat])
        sent(many(pl.ds(0, 3), mat, n_y), sib_send.at[mat])

    def reduce_second(i, carry):
        k = wide - 2 - i
        for m in range(SUBS):
            part = pl.ds(m * sub, sub)
            rs2_copy(s2, k + 1, m).wait_recv()
            s2[k, part, :] = (
                s2[k, part, :].astype(F32) + p2[k, part, :].astype(F32)
            ).astype(BF16)
            rs2_copy(s2, k, m).start()
            second_quarter(k - 1, m, 0, rows)
        return carry

    if wide > 2:
        lax.fori_loop(0, wide - 2, reduce_second, 0)
    else:
        for q in range(4):
            second_quarter(0, q, 0, rows)

    for m in range(SUBS):
        part = pl.ds(m * sub, sub)
        rs2_copy(s2, 1, m).wait_recv()
        total = s2[0, part, :].astype(F32) + p2[0, part, :].astype(F32)
        out[part, :] = (mid[part, :].astype(F32) + 0.5 * total).astype(BF16)

    sent(s2, rs2_send)


def solution(mesh):
    n_x = mesh.shape["tp"]
    n_y = mesh.shape["fs"] // CORES

    def local(stream, gain1, g1, u1, d1, gain2, g2, u2, d2):
        rows, feats = stream.shape
        shard, ff = g1.shape
        wide = n_x // 2
        any_spec = pl.BlockSpec(memory_space=pl.ANY)
        vmem_spec = pl.BlockSpec(memory_space=pltpu.VMEM)
        dma = pltpu.SemaphoreType.DMA
        y_count = 9 * (n_y - 1)
        return pl.pallas_call(
            functools.partial(kernel, n_x, n_y),
            out_shape=pltpu.VMEM((rows, feats), BF16),
            in_specs=[any_spec] * 9,
            out_specs=vmem_spec,
            scratch_shapes=[
                pltpu.VMEM((3, feats, ff), BF16),
                pltpu.VMEM((3, feats, ff), BF16),
                pltpu.VMEM((3, ff, feats), BF16),
                pltpu.VMEM((rows, feats), BF16),
                pltpu.VMEM((n_x, rows, feats), BF16),
                pltpu.VMEM((n_x, rows, feats), BF16),
                pltpu.VMEM((n_x - 1, rows, feats), BF16),
                pltpu.VMEM((rows, feats), BF16),
                pltpu.VMEM((wide, rows, feats), BF16),
                pltpu.VMEM((wide, rows, feats), BF16),
                pltpu.VMEM((wide - 1, rows, feats), BF16),
                pltpu.VMEM((shard, ff), BF16),
                pltpu.VMEM((shard, ff), BF16),
                pltpu.VMEM((ff, shard), BF16),
                pltpu.VMEM((2, rows, ff), BF16),
                pltpu.VMEM((2, feats // LANES, LANES), BF16),
                pltpu.VMEM((2, 1, feats), F32),
                dma((9,)),
                dma((2 * SUBS,)),
                dma((y_count,)),
                dma((9,)),
                dma((3,)),
                dma((3,)),
                dma,
                dma,
                dma,
                dma,
                dma((3,)),
                dma((3,)),
                dma((3,)),
                dma((3,)),
                pltpu.SemaphoreType.REGULAR,
                pltpu.SemaphoreType.REGULAR,
            ],
            compiler_params=pltpu.CompilerParams(
                collective_id=0, has_side_effects=True, vmem_limit_bytes=60 * 1024 * 1024
            ),
        )(stream, gain1.reshape(-1, LANES), g1, u1, d1, gain2.reshape(-1, LANES), g2, u2, d2)

    tokens = P(("grp", "fs", "tp"), None)
    rows_split, cols_split = P("fs", "tp"), P("tp", "fs")
    in_specs = (
        tokens,
        P(), rows_split, rows_split, cols_split,
        P(), rows_split, rows_split, cols_split,
    )
    return jax.shard_map(local, mesh=mesh, in_specs=in_specs, out_specs=tokens, check_vma=False)
```
